256 devices in a mesh: sp: 16 (over y, x), dp: 16 (over z, core).
Axes of the slice: x: 4, y: 4, z: 8, core: 2. Of those that a mesh axis runs over, the one named last changes fastest.
Arguments:
- tokens: bfloat16 [16, 4096, 2048], P('dp', 'sp'), may hold values from -200 to 200
- w_qdown: bfloat16 [2048, 512], P('dp'), may hold values from -0.125 to 0.125
- w_kvdown: bfloat16 [2048, 512], P('dp'), may hold values from -0.125 to 0.125
- w_rotary: bfloat16 [2048, 64], replicated, may hold values from -0.125 to 0.125
- q_gain: float32 [512], replicated, may hold values from 0.1 to 1.9
- kv_gain: float32 [512], replicated, may hold values from 0.1 to 1.9
- w_qup: bfloat16 [512, 3072], P('dp'), may hold values from -1 to 1
- w_kvup: bfloat16 [512, 4096], P('dp'), may hold values from -1 to 1
- w_out: bfloat16 [2048, 2048], P(None, 'dp'), may hold values from -0.125 to 0.125
- out_gain: float32 [2048], replicated, may hold values from 0.1 to 1.9
Outputs:
- mixed: bfloat16 [16, 4096, 2048], P('dp', 'sp')
The draws below stay inside these ranges and needn't reach their ends.
All inputs are finite; a program needn't handle non-finite values.
Results may differ from the reference program's by a relative error of at most 0.01.
The reference program's roundings to bfloat16 on the way count: a program that leaves them out, or rounds other values in their place, can miss the bound.
Values may be sent and summed in bfloat16 or wider, within the bound.
A program may use at most 128 MiB of HBM per device.

```python
import math
import jax
import jax.numpy as jnp
from jax import lax

D = 2048
HEADS = 16
Q_RANK = 512
KV_RANK = 512
NOPE = 128
ROPE = 64
VDIM = 128
LENGTH = 4096
BATCH = 16


def draw_tokens(key, part):
    value_key = jax.random.fold_in(key, 11)
    values = jnp.clip(jax.random.normal(value_key, (BATCH, LENGTH, D), jnp.float32), -6.0, 6.0)
    return values.astype(jnp.bfloat16)


def base_weight(key, salt, rank, width):
    normal = jax.random.normal(jax.random.fold_in(key, salt), (rank, HEADS, width), jnp.float32)
    return jnp.clip(normal, -4.0, 4.0) * rank ** (-0.5)


def draw_w_qup(key, part):
    values = base_weight(key, 41, Q_RANK, NOPE + ROPE)
    values = jnp.clip(values, -1.0, 1.0)
    return values.reshape(Q_RANK, HEADS * (NOPE + ROPE)).astype(jnp.bfloat16)


def draw_w_kvup(key, part):
    values = base_weight(key, 51, KV_RANK, NOPE + VDIM)
    values = jnp.clip(values, -1.0, 1.0)
    return values.reshape(KV_RANK, HEADS * (NOPE + VDIM)).astype(jnp.bfloat16)


def levels(rng, extent, split, least, largest):
    def one(axis_at, blocks):
        draws = jax.random.uniform(jax.random.fold_in(jax.random.fold_in(rng, 6), axis_at), (blocks,), jnp.float32, least / len(split), largest / len(split))
        return jnp.repeat(jnp.exp(draws), extent[axis_at] // blocks).reshape((-1,) + (1,) * (len(extent) - axis_at - 1))

    level = one(*split[0])
    for cut in split[1:]:
        level = level * one(*cut)
    return level


def centred(stream_key, extent, scale, reach, cuts=(), dtype=jnp.bfloat16):
    factor_of = levels(stream_key, extent, cuts, -0.22, 0.18) if cuts else 1.0
    result = jax.random.normal(stream_key, extent, jnp.float32) * scale * factor_of
    return jnp.minimum(jnp.maximum(result, -reach), reach).astype(dtype)


def setup_inputs(seed: int = 0) -> dict:
    arg_keys = jax.random.split(jax.random.key(seed), 11)
    return {
        "tokens": draw_tokens(jax.random.fold_in(arg_keys[10], 71), 0),
        "w_qdown": centred(arg_keys[1], (D, Q_RANK), D ** -0.5, 0.125, ((0, 16),)),
        "w_kvdown": centred(arg_keys[2], (D, KV_RANK), D ** -0.5, 0.125, ((0, 16),)),
        "w_rotary": centred(arg_keys[3], (D, ROPE), D ** -0.5, 0.125),
        "q_gain": jnp.clip(1.0 + 0.18 * jax.random.normal(arg_keys[4], (Q_RANK,), jnp.float32), 0.1, 1.9),
        "kv_gain": jnp.clip(1.0 + 0.18 * jax.random.normal(arg_keys[5], (KV_RANK,), jnp.float32), 0.1, 1.9),
        "w_qup": draw_w_qup(jax.random.fold_in(arg_keys[10], 71), 0),
        "w_kvup": draw_w_kvup(jax.random.fold_in(arg_keys[10], 71), 0),
        "w_out": centred(arg_keys[8], (HEADS * VDIM, D), (HEADS * VDIM) ** -0.5, 0.125, ((1, 16),)),
        "out_gain": jnp.clip(1.0 + 0.18 * jax.random.normal(arg_keys[9], (D,), jnp.float32), 0.1, 1.9),
    }


EPSILON = 1e-06
THETA = 10000.0

def norm_rows(values, gain):
    scale = lax.rsqrt(lax.optimization_barrier(jnp.mean(values * values, axis=-1, keepdims=True)) + EPSILON)
    return values * scale * gain

def rotate(values, cosine, sine):
    half = values.shape[-1] // 2
    first = values[..., :half]
    second = values[..., half:]
    return jnp.concatenate([first * cosine - second * sine, second * cosine + first * sine], axis=-1)

def reference(tokens, w_qdown, w_kvdown, w_rotary, q_gain, kv_gain, w_qup, w_kvup, w_out, out_gain):
    length = tokens.shape[1]
    positions = jnp.arange(length).astype(jnp.float32)
    freqs = THETA ** (-jnp.arange(0, ROPE, 2).astype(jnp.float32) / ROPE)
    angles = positions[:, None] * freqs[None, :]
    cosine = jnp.cos(angles)
    sine = jnp.sin(angles)
    block = math.gcd(length, 512)
    qk_width = NOPE + ROPE
    scaling = qk_width ** (-0.5)

    def one_sequence(sequence):
        q_lat = jnp.dot(sequence, w_qdown, preferred_element_type=jnp.float32)
        kv_lat = jnp.dot(sequence, w_kvdown, preferred_element_type=jnp.float32)
        q_norm = norm_rows(q_lat, q_gain).astype(jnp.bfloat16)
        kv_norm = norm_rows(kv_lat, kv_gain).astype(jnp.bfloat16)
        key_rot = rotate(jnp.dot(sequence, w_rotary, preferred_element_type=jnp.float32), cosine, sine).astype(jnp.bfloat16)
        q_full = jnp.dot(q_norm, w_qup, preferred_element_type=jnp.float32).reshape(length, HEADS, qk_width)
        q_turn = rotate(q_full[..., NOPE:], cosine[:, None, :], sine[:, None, :])
        queries = jnp.concatenate([q_full[..., :NOPE], q_turn], axis=-1).astype(jnp.bfloat16)
        keyval = jnp.dot(kv_norm, w_kvup, preferred_element_type=jnp.float32).astype(jnp.bfloat16)
        keyval = keyval.reshape(length, HEADS, NOPE + VDIM)
        keys_all = keyval[..., :NOPE].astype(jnp.float32)
        values_all = keyval[..., NOPE:].astype(jnp.float32)
        rot_all = key_rot.astype(jnp.float32)
        outputs = []
        for begin in range(0, length, block):
            finish = begin + block
            query_block = queries[begin:finish].astype(jnp.float32)
            scores = jnp.einsum('qhd,khd->hqk', query_block[..., :NOPE], keys_all[:finish])
            scores = scores + jnp.einsum('qhd,kd->hqk', query_block[..., NOPE:], rot_all[:finish])
            scores = scores * scaling
            query_pos = begin + jnp.arange(block)
            key_pos = jnp.arange(finish)
            allowed = key_pos[None, :] <= query_pos[:, None]
            scores = jnp.where(allowed[None], scores, -jnp.inf)
            top = lax.optimization_barrier(jnp.max(scores, axis=-1, keepdims=True))
            expo = jnp.exp(scores - top)
            weights = (expo / lax.optimization_barrier(jnp.sum(expo, axis=-1, keepdims=True))).astype(jnp.bfloat16)
            attended = jnp.einsum('hqk,khd->qhd', weights.astype(jnp.float32), values_all[:finish])
            outputs.append(attended.astype(jnp.bfloat16))
        attended_all = jnp.concatenate(outputs, axis=0).reshape(length, HEADS * VDIM)
        proj = jnp.dot(attended_all, w_out, preferred_element_type=jnp.float32)
        return norm_rows(proj, out_gain).astype(jnp.bfloat16)
    return lax.map(one_sequence, tokens)
```

```python
import functools

import jax
import jax.numpy as jnp
import numpy as np
from jax import lax
from jax.experimental import pallas as pl
from jax.experimental.pallas import tpu as pltpu
from jax.sharding import PartitionSpec as P

HEADS = 16
NOPE = 128
ROPE = 64
VDIM = 128
D = 2048
RANK = 512
LENGTH = 4096
BLOCK = 256
EPSILON = 1e-06
THETA = 10000.0
LOG2E = 1.4426950408889634
SCALE = (NOPE + ROPE) ** (-0.5) * LOG2E
MESH = pl.DeviceIdType.MESH
BF16 = jnp.bfloat16
F32 = jnp.float32
Q_WIDTH = 4 * NOPE
R_WIDTH = 4 * ROPE
UP_WIDTH = Q_WIDTH + R_WIDTH + 4 * (NOPE + VDIM)
A_ROWS = 96
KV_ROWS = BLOCK + 32


def turn_table():
    positions = np.arange(LENGTH).astype(np.float32)
    freqs = np.float32(THETA) ** (-np.arange(0, ROPE, 2).astype(np.float32) / np.float32(ROPE))
    angles = positions[:, None] * freqs[None, :].astype(np.float32)
    cosine, sine = np.cos(angles), np.sin(angles)
    return np.concatenate([cosine, cosine, -sine, sine], axis=1).astype(np.float32)


def dot(a, b):
    return jnp.dot(a, b, preferred_element_type=F32)


def kernel(
    tok_hbm, wq_hbm, wkv_hbm, wrot, q_gain, kv_gain, wqup_hbm, wkvup_hbm, wout_hbm, out_gain, tab_hbm,
    out_ref,
    tk, pt, lhs, wd, part_send, part_recv, kvb, qb, wqs, wup, wo, tab, kcat, vbuf, qcat, acc, mbuf, lbuf,
    osend, orecv, send_sems, recv_sems, local_sems,
):
    sp, dp = lax.axis_index("sp"), lax.axis_index("dp")
    y, x = lax.div(sp, 4), lax.rem(sp, 4)
    z, c = lax.div(dp, 2), lax.rem(dp, 2)

    def m4(v):
        return lax.rem(v + 8, 4)

    def m8(v):
        return lax.rem(v + 16, 8)

    def plane(yy, xx):
        return (m4(yy) * 4 + m4(xx), dp)

    def along(zz):
        return (sp, m8(zz) * 2 + c)

    partner = (sp, z * 2 + (1 - c))
    xp, xm, yp, ym = plane(y, x + 1), plane(y, x - 1), plane(y + 1, x), plane(y - 1, x)
    zp, zm = along(z + 1), along(z - 1)

    local = [
        pltpu.make_async_copy(wq_hbm, wd.at[z, :, pl.ds(0, RANK)], local_sems.at[0]),
        pltpu.make_async_copy(wkv_hbm, wd.at[z, :, pl.ds(RANK, RANK)], local_sems.at[1]),
        pltpu.make_async_copy(tok_hbm, tk, local_sems.at[2]),
        pltpu.make_async_copy(
            wqup_hbm.at[:, pl.ds(pl.multiple_of(y * 768, 128), 768)], wqs, local_sems.at[3]
        ),
        pltpu.make_async_copy(
            wkvup_hbm.at[:, pl.ds(pl.multiple_of(y * 1024, 128), 1024)],
            wup.at[dp, :, pl.ds(Q_WIDTH + R_WIDTH, 1024)],
            local_sems.at[4],
        ),
        pltpu.make_async_copy(
            wout_hbm, wo.at[:, pl.ds(pl.multiple_of(dp * 128, 128), 128)], local_sems.at[5]
        ),
    ]
    for i in range(4):
        local.append(
            pltpu.make_async_copy(
                tab_hbm.at[pl.ds(pl.multiple_of(i * 1024 + x * 256, 256), 256)], tab.at[i], local_sems.at[6 + i]
            )
        )
    for copy in local:
        copy.start()

    barrier = pltpu.get_barrier_semaphore()
    for peer in (xp, xm, yp, ym, plane(y + 2, x), zp, zm, partner):
        pl.semaphore_signal(barrier, inc=1, device_id=peer, device_id_type=MESH)
    pl.semaphore_wait(barrier, 8)

    count = [0]
    started = []

    def remote(src, dst, peer, incoming):
        k = count[0]
        count[0] += 1
        out = pltpu.make_async_remote_copy(
            src_ref=src, dst_ref=dst, send_sem=send_sems.at[k], recv_sem=recv_sems.at[k],
            device_id=peer, device_id_type=MESH,
        )
        into = pltpu.make_async_remote_copy(
            src_ref=incoming, dst_ref=incoming, send_sem=send_sems.at[k], recv_sem=recv_sems.at[k],
            device_id=peer, device_id_type=MESH,
        )
        out.start()
        started.append(out)
        return into.wait_recv

    colour = m4(x + 2 * y)

    def quarter(zo, q, part=None):
        if part is None:
            return wd.at[m8(zo), pl.ds(pl.multiple_of(m4(q) * 32, 32), 32)]
        return wd.at[m8(zo), pl.ds(pl.multiple_of(m4(q) * 32 + 16 * part, 16), 16)]

    def ring(view):
        def start(step):
            if step < 4:
                a = remote(view(z - step + 1), view(z - step + 1), zp, view(z - step))
                b = remote(view(z + step - 1), view(z + step - 1), zm, view(z + step))
            else:
                a = remote(view(z - 3, 0), view(z - 3, 0), zp, view(z - 4, 0))
                b = remote(view(z + 3, 1), view(z + 3, 1), zm, view(z + 4, 1))
            return a, b

        return start

    local[0].wait()
    local[1].wait()
    down_ring = ring(lambda zo, part=None: quarter(zo, colour, part))
    waits = down_ring(1)
    local[2].wait()
    tokens_in = remote(tk, pt, partner, pt)
    sides = []

    def share(zo):
        own = quarter(zo, colour)
        sides.append(remote(own, own, xp, quarter(zo, colour - 1)))
        sides.append(remote(own, own, xm, quarter(zo, colour + 1)))
        for peer, part in ((yp, 0), (ym, 1)):
            half = quarter(zo, colour, part)
            sides.append(remote(half, half, peer, quarter(zo, colour + 2, part)))

    local[3].wait()
    for h in range(4):
        wup[dp, :, NOPE * h : NOPE * (h + 1)] = wqs[:, 192 * h : 192 * h + NOPE]
    wup[dp, :, Q_WIDTH : Q_WIDTH + R_WIDTH] = jnp.concatenate(
        [wqs[:, 192 * h + NOPE : 192 * (h + 1)] for h in range(4)], axis=1
    )
    for copy in local[6:10]:
        copy.wait()
    own_tab = tab[y]
    kr = dot(tk[...], wrot[...])
    kr_swap = jnp.concatenate([kr[:, 32:], kr[:, :32]], axis=1)
    kr = (kr * own_tab[:, :64] + kr_swap * own_tab[:, 64:]).astype(BF16)
    packed = jnp.concatenate([kr[:128], kr[128:]], axis=1)
    for t in range(4):
        kvb[sp, BLOCK:KV_ROWS, 128 * t : 128 * (t + 1)] = packed[32 * t : 32 * (t + 1)]

    for step in range(1, 5):
        for wait in waits:
            wait()
        if step < 4:
            waits = down_ring(step + 1)
            share(z - step)
            share(z + step)
        else:
            share(z + 4)
        if step == 1:
            tokens_in()
            for zo in range(8):
                columns = pl.ds(pl.multiple_of(256 * zo + 128 * c, 128), 128)
                lhs[0:256, 128 * zo : 128 * (zo + 1)] = tk[:, columns]
                lhs[256:512, 128 * zo : 128 * (zo + 1)] = pt[:, columns]

    local[4].wait()

    def up_block(zo, part=None, core=c):
        if part is None:
            return wup.at[m8(zo) * 2 + core]
        return wup.at[m8(zo) * 2 + core, pl.ds(16 * part, 16)]

    up_ring = ring(up_block)
    handed = []

    def hand_up(zo):
        handed.append(remote(up_block(zo), up_block(zo), partner, up_block(zo, core=1 - c)))

    up_waits = up_ring(1)
    hand_up(z)

    for wait in sides:
        wait()
    weights = wd[...].reshape(1024, 1024)
    part_send[...] = dot(lhs[256:512], weights)
    partial_in = remote(part_send, part_recv, partner, part_recv)
    own = dot(lhs[0:256], weights)
    partial_in()
    own = own + part_recv[...]

    def norm(v, gain):
        return v * lax.rsqrt(jnp.mean(v * v, axis=-1, keepdims=True) + EPSILON) * gain

    kvb[sp, 0:BLOCK, :] = norm(own[:, RANK:], kv_gain[...]).astype(BF16)
    qb[y] = norm(own[:, :RANK], q_gain[...]).astype(BF16)

    mid_a, mid_b = A_ROWS // 2, A_ROWS + (KV_ROWS - A_ROWS) // 2

    def rows_of(oy, ox, lo, hi):
        return kvb.at[m4(oy) * 4 + m4(ox), pl.ds(lo, hi - lo)]

    def a_piece(oy, ox, part=None):
        lo, hi = ((0, A_ROWS), (0, mid_a), (mid_a, A_ROWS))[0 if part is None else part + 1]
        return rows_of(oy, ox, lo, hi)

    def b_piece(oy, ox, part=None):
        lo, hi = ((A_ROWS, KV_ROWS), (A_ROWS, mid_b), (mid_b, KV_ROWS))[0 if part is None else part + 1]
        return rows_of(oy, ox, lo, hi)

    def q_piece(oy, ox, part=None):
        if part is None:
            return qb.at[m4(oy)]
        return qb.at[m4(oy), pl.ds(128 * part, 128)]

    def x_first(piece, oy):
        return (
            remote(piece(oy, x), piece(oy, x), xp, piece(oy, x - 1)),
            remote(piece(oy, x), piece(oy, x), xm, piece(oy, x + 1)),
        )

    def x_second(piece, oy):
        return (
            remote(piece(oy, x - 1, 0), piece(oy, x - 1, 0), xp, piece(oy, x - 2, 0)),
            remote(piece(oy, x + 1, 1), piece(oy, x + 1, 1), xm, piece(oy, x + 2, 1)),
        )

    def y_first(piece, ox):
        return (
            remote(piece(y, ox), piece(y, ox), yp, piece(y - 1, ox)),
            remote(piece(y, ox), piece(y, ox), ym, piece(y + 1, ox)),
        )

    def y_second(piece, ox):
        return (
            remote(piece(y - 1, ox, 0), piece(y - 1, ox, 0), yp, piece(y - 2, ox, 0)),
            remote(piece(y + 1, ox, 1), piece(y + 1, ox, 1), ym, piece(y + 2, ox, 1)),
        )

    def wait_all(waits):
        for wait in waits:
            wait()

    def up_step(step):
        wait_all(up_waits)
        nxt = up_ring(step + 1) if step < 4 else ()
        if step < 4:
            hand_up(z - step)
            hand_up(z + step)
        else:
            hand_up(z + 4)
        return nxt

    ax1 = x_first(a_piece, y)
    by1 = y_first(b_piece, x)
    bx1 = {0: x_first(b_piece, y)}
    qy1 = y_first(q_piece, x)
    ay1 = {0: y_first(a_piece, x)}
    bx2, ay2 = {}, {}

    local[5].wait()

    def out_view(chunk, core=c):
        def view(zo, part=None):
            lo, size = (1024 * chunk, 1024) if part is None else (1024 * chunk + 512 * part, 512)
            return wo.at[pl.ds(lo, size), pl.ds(pl.multiple_of(m8(zo) * 256 + core * 128, 128), 128)]

        return view

    out_rings = [ring(out_view(chunk)) for chunk in range(2)]
    out_waits = [None, None]

    def hand_out(chunk, zo):
        mine, other = out_view(chunk)(zo), out_view(chunk, 1 - c)(zo)
        handed.append(remote(mine, mine, partner, other))

    def out_start():
        for chunk in range(2):
            out_waits[chunk] = out_rings[chunk](1)
            hand_out(chunk, z)

    def out_step(step):
        for chunk in range(2):
            wait_all(out_waits[chunk])
            if step < 4:
                out_waits[chunk] = out_rings[chunk](step + 1)
                hand_out(chunk, z - step)
                hand_out(chunk, z + step)
            else:
                hand_out(chunk, z + 4)

    wait_all(ax1)
    ax2 = x_second(a_piece, y)
    ay1[-1] = y_first(a_piece, x - 1)
    ay1[1] = y_first(a_piece, x + 1)
    wait_all(by1)
    by2 = y_second(b_piece, x)
    bx1[-1] = x_first(b_piece, y - 1)
    bx1[1] = x_first(b_piece, y + 1)
    wait_all(bx1[0])
    bx2[0] = x_second(b_piece, y)
    up_waits = up_step(1)
    wait_all(qy1)
    qy2 = y_second(q_piece, x)
    wait_all(ax2)
    ay1[2] = y_first(a_piece, x + 2)
    wait_all(ay1[0])
    ay2[0] = y_second(a_piece, x)
    up_waits = up_step(2)
    wait_all(by2)
    bx1[2] = x_first(b_piece, y + 2)
    wait_all(bx2[0])
    up_waits = up_step(3)
    up_step(4)
    out_start()
    wait_all(handed[:8])
    del handed[:8]
    wait_all(ay1[-1])
    ay2[-1] = y_second(a_piece, x - 1)
    wait_all(ay1[1])
    ay2[1] = y_second(a_piece, x + 1)

    lane = lax.broadcasted_iota(jnp.int32, (256, 256), 1)
    first_half = lax.rem(lane, 64) < 32
    low = lax.rem(lax.broadcasted_iota(jnp.int32, (256, 128), 1), 128) < 64

    def expand_queries(i):
        up = dot(qb[i], wup[:, :, 0 : Q_WIDTH + R_WIDTH].reshape(RANK, Q_WIDTH + R_WIDTH))
        table = tab[i]
        cosine = jnp.concatenate([table[:, :64]] * 4, axis=1)
        sine = jnp.concatenate([table[:, 64:]] * 4, axis=1)
        u = up[:, Q_WIDTH:]
        swapped = jnp.where(first_half, pltpu.roll(u, R_WIDTH - 32, 1), pltpu.roll(u, 32, 1))
        turned = u * cosine + swapped * sine
        for h in range(4):
            qcat[h, i, :, 0:NOPE] = up[:, NOPE * h : NOPE * (h + 1)].astype(BF16)
            pair = turned[:, 128 * (h // 2) : 128 * (h // 2 + 1)]
            keep = low if h % 2 == 0 else jnp.logical_not(low)
            qcat[h, i, :, NOPE:256] = jnp.where(keep, pair, 0.0).astype(BF16)

    def expand_keys(o):
        up = dot(kvb[o, 0:BLOCK, :], wup[:, :, Q_WIDTH + R_WIDTH :].reshape(RANK, 1024)).astype(BF16)
        for h in range(4):
            kcat[h, o, :, 0:NOPE] = up[:, 256 * h : 256 * h + NOPE]
            vbuf[h, o] = up[:, 256 * h + NOPE : 256 * (h + 1)]
        for t in range(4):
            pair = kvb[o, BLOCK:KV_ROWS, 128 * t : 128 * (t + 1)].astype(F32)
            turned = pltpu.roll(pair, 64, 1)
            first = jnp.where(low[:32], pair, turned).astype(BF16)
            second = jnp.where(low[:32], turned, pair).astype(BF16)
            for h in range(4):
                kcat[h, o, 32 * t : 32 * (t + 1), NOPE:256] = first
                kcat[h, o, 128 + 32 * t : 128 + 32 * (t + 1), NOPE:256] = second

    def expand_row(r):
        def step(j, carry):
            expand_keys(r * 4 + j)
            return carry

        lax.fori_loop(0, 4, step, 0)

    def attend(i, r, masked):
        def pair(g, carry):
            for h in (2 * g, 2 * g + 1):
                k = kcat[h, pl.ds(4 * r, 4)].reshape(1024, 256)
                v = vbuf[h, pl.ds(4 * r, 4)].reshape(1024, VDIM)
                s = lax.dot_general(qcat[h, i], k, (((1,), (1,)), ((), ())), preferred_element_type=F32)
                s = s * SCALE
                if masked:
                    q_pos = lax.broadcasted_iota(jnp.int32, (256, 1024), 0) + x * 256
                    k_pos = lax.broadcasted_iota(jnp.int32, (256, 1024), 1)
                    s = jnp.where(k_pos <= q_pos, s, -jnp.inf)
                old = mbuf[h, i]
                top = jnp.maximum(old, jnp.max(s, axis=-1, keepdims=True))
                p = jnp.exp2(s - top[:, :1])
                alpha = jnp.exp2(old - top)
                mbuf[h, i] = top
                lbuf[h, i] = lbuf[h, i] * alpha + jnp.sum(p, axis=-1, keepdims=True)
                acc[h, i] = acc[h, i] * alpha + dot(p.astype(BF16), v)
            return carry

        lax.fori_loop(0, 2, pair, 0)

    def attend_row(r):
        attend(r, r, True)

        def step(i, carry):
            attend(i, r, False)
            return carry

        lax.fori_loop(r + 1, 4, step, 0)

    acc[...] = jnp.zeros_like(acc)
    lbuf[...] = jnp.zeros_like(lbuf)
    mbuf[...] = jnp.full_like(mbuf, -jnp.inf)

    wait_all(qy2)

    def expand_query_block(i, carry):
        expand_queries(i)
        return carry

    lax.fori_loop(0, 4, expand_query_block, 0)
    expand_row(y)
    wait_all(bx1[1])
    bx2[1] = x_second(b_piece, y + 1)
    wait_all(bx1[-1])
    bx2[-1] = x_second(b_piece, y - 1)
    wait_all(ay1[2])
    ay2[2] = y_second(a_piece, x + 2)
    attend_row(y)
    out_step(1)
    wait_all(bx1[2])
    bx2[2] = x_second(b_piece, y + 2)
    wait_all(bx2[1])
    expand_row(m4(y + 1))
    attend_row(m4(y + 1))
    out_step(2)
    wait_all(bx2[-1])
    expand_row(m4(y - 1))
    attend_row(m4(y - 1))
    out_step(3)
    for delta in (0, -1, 1, 2):
        wait_all(ay2[delta])
    wait_all(bx2[2])
    expand_row(m4(y + 2))
    attend_row(m4(y + 2))

    def finish(i, carry):
        for h in range(4):
            osend[i, :, VDIM * h : VDIM * (h + 1)] = (acc[h, i] / lbuf[h, i]).astype(BF16)
        return carry

    lax.fori_loop(0, 4, finish, 0)
    back = []
    for delta in (2, 1, 3):
        back.append(
            remote(osend.at[m4(y + delta)], orecv.at[y], plane(y + delta, x), orecv.at[m4(y - delta)])
        )
    orecv[y] = osend[y]
    out_step(4)
    wait_all(handed)
    wait_all(back)

    def project(j, total):
        return total + dot(orecv[j], wo[pl.ds(pl.multiple_of(512 * j, 512), 512), :])

    total = jnp.zeros((BLOCK, D), F32)
    for j in range(4):
        total = project(j, total)
    out_ref[...] = norm(total, out_gain[...]).astype(BF16)
    for copy in started:
        copy.wait_send()


N_COPIES = 176


def body(tokens, w_qdown, w_kvdown, w_rotary, q_gain, kv_gain, w_qup, w_kvup, w_out, out_gain):
    table = jnp.asarray(turn_table())
    any_spec = pl.BlockSpec(memory_space=pl.ANY)
    vmem_spec = pl.BlockSpec(memory_space=pltpu.VMEM)
    call = pl.pallas_call(
        kernel,
        out_shape=jax.ShapeDtypeStruct((BLOCK, D), BF16),
        in_specs=[any_spec, any_spec, any_spec, vmem_spec, vmem_spec, vmem_spec]
        + [any_spec, any_spec, any_spec, vmem_spec, any_spec],
        out_specs=vmem_spec,
        scratch_shapes=[
            pltpu.VMEM((BLOCK, D), BF16),
            pltpu.VMEM((BLOCK, D), BF16),
            pltpu.VMEM((2 * BLOCK, 1024), BF16),
            pltpu.VMEM((8, 128, 1024), BF16),
            pltpu.VMEM((BLOCK, 1024), F32),
            pltpu.VMEM((BLOCK, 1024), F32),
            pltpu.VMEM((16, KV_ROWS, RANK), BF16),
            pltpu.VMEM((4, BLOCK, RANK), BF16),
            pltpu.VMEM((32, 768), BF16),
            pltpu.VMEM((16, 32, UP_WIDTH), BF16),
            pltpu.VMEM((D, D), BF16),
            pltpu.VMEM((4, BLOCK, 128), F32),
            pltpu.VMEM((4, 16, BLOCK, 256), BF16),
            pltpu.VMEM((4, 16, BLOCK, VDIM), BF16),
            pltpu.VMEM((4, 4, BLOCK, 256), BF16),
            pltpu.VMEM((4, 4, BLOCK, VDIM), F32),
            pltpu.VMEM((4, 4, BLOCK, 128), F32),
            pltpu.VMEM((4, 4, BLOCK, 128), F32),
            pltpu.VMEM((4, BLOCK, 512), BF16),
            pltpu.VMEM((4, BLOCK, 512), BF16),
            pltpu.SemaphoreType.DMA((N_COPIES,)),
            pltpu.SemaphoreType.DMA((N_COPIES,)),
            pltpu.SemaphoreType.DMA((10,)),
        ],
        compiler_params=pltpu.CompilerParams(
            collective_id=0, has_side_effects=True, vmem_limit_bytes=63 * 1024 * 1024
        ),
        name="latent_attention",
    )
    mixed = call(
        tokens[0], w_qdown, w_kvdown, w_rotary, q_gain[None], kv_gain[None],
        w_qup, w_kvup, w_out, out_gain[None], table,
    )
    return mixed[None]


def solution(mesh):
    in_specs = (
        P("dp", "sp", None),
        P("dp", None),
        P("dp", None),
        P(),
        P(),
        P(),
        P("dp", None),
        P("dp", None),
        P(None, "dp"),
        P(),
    )
    out_specs = P("dp", "sp", None)
    return jax.shard_map(body, mesh=mesh, in_specs=in_specs, out_specs=out_specs, check_vma=False)
```

```python
import functools

import jax
import jax.numpy as jnp
import numpy as np
from jax import lax
from jax.experimental import pallas as pl
from jax.experimental.pallas import tpu as pltpu
from jax.sharding import PartitionSpec as P

HEADS = 16
NOPE = 128
ROPE = 64
VDIM = 128
D = 2048
RANK = 512
LENGTH = 4096
BLOCK = 256
EPSILON = 1e-06
THETA = 10000.0
LOG2E = 1.4426950408889634
SCALE = (NOPE + ROPE) ** (-0.5) * LOG2E
MESH = pl.DeviceIdType.MESH
BF16 = jnp.bfloat16
F32 = jnp.float32
Q_WIDTH = 4 * NOPE
R_WIDTH = 4 * ROPE
UP_WIDTH = Q_WIDTH + R_WIDTH + 4 * (NOPE + VDIM)
A_ROWS = 96
KV_ROWS = BLOCK + 32


def turn_table():
    positions = np.arange(LENGTH).astype(np.float32)
    freqs = np.float32(THETA) ** (-np.arange(0, ROPE, 2).astype(np.float32) / np.float32(ROPE))
    angles = positions[:, None] * freqs[None, :].astype(np.float32)
    cosine, sine = np.cos(angles), np.sin(angles)
    return np.concatenate([cosine, cosine, -sine, sine], axis=1).astype(np.float32)


def dot(a, b):
    return jnp.dot(a, b, preferred_element_type=F32)


class Move:
    def __init__(self, sems, src, dst, peer, incoming):
        def make(a, b):
            return pltpu.make_async_remote_copy(
                src_ref=a, dst_ref=b, send_sem=sems[0], recv_sem=sems[1], device_id=peer, device_id_type=MESH
            )

        self.out, self.into = make(src, dst), make(incoming, incoming)

    def start(self):
        self.out.start()

    def wait(self):
        self.into.wait_recv()

    def finish(self):
        self.out.wait_send()


def start_all(moves):
    for move in moves:
        move.start()


def wait_all(moves):
    for move in moves:
        move.wait()


def norm(v, gain):
    return v * lax.rsqrt(jnp.mean(v * v, axis=-1, keepdims=True) + EPSILON) * gain


def kernel(
    tok_hbm, wq_hbm, wkv_hbm, wrot_hbm, q_gain, kv_gain, wqup_hbm, wkvup_hbm, wout_hbm, out_gain, tab_hbm,
    out_ref,
    tk, pt, lhs, wd, part_send, part_recv, kvb, qb, wqs, wup, wo, wrot, tab, kcat, vbuf, qcat, acc, mbuf,
    osend, orecv, send_sems, recv_sems, local_sems,
):
    sp, dp = lax.axis_index("sp"), lax.axis_index("dp")
    y, x = lax.div(sp, 4), lax.rem(sp, 4)
    z, c = lax.div(dp, 2), lax.rem(dp, 2)

    def m4(v):
        return lax.rem(v + 8, 4)

    def m8(v):
        return lax.rem(v + 16, 8)

    def plane(yy, xx):
        return (m4(yy) * 4 + m4(xx), dp)

    def along(zz):
        return (sp, m8(zz) * 2 + c)

    partner = (sp, z * 2 + (1 - c))
    xp, xm, yp, ym = plane(y, x + 1), plane(y, x - 1), plane(y + 1, x), plane(y - 1, x)
    zp, zm = along(z + 1), along(z - 1)

    local = [
        pltpu.make_async_copy(wkv_hbm, wd.at[z, :, pl.ds(0, RANK)], local_sems.at[0]),
        pltpu.make_async_copy(wq_hbm, wd.at[z, :, pl.ds(RANK, RANK)], local_sems.at[1]),
        pltpu.make_async_copy(tok_hbm, tk, local_sems.at[2]),
        pltpu.make_async_copy(
            wqup_hbm.at[:, pl.ds(pl.multiple_of(y * 768, 128), 768)], wqs, local_sems.at[3]
        ),
        pltpu.make_async_copy(
            wkvup_hbm.at[:, pl.ds(pl.multiple_of(y * 1024, 128), 1024)],
            wup.at[dp, :, pl.ds(Q_WIDTH + R_WIDTH, 1024)],
            local_sems.at[4],
        ),
        pltpu.make_async_copy(
            wout_hbm, wo.at[:, pl.ds(pl.multiple_of(dp * 128, 128), 128)], local_sems.at[5]
        ),
        pltpu.make_async_copy(wrot_hbm, wrot, local_sems.at[6]),
    ]
    for i in range(4):
        local.append(
            pltpu.make_async_copy(
                tab_hbm.at[pl.ds(pl.multiple_of(i * 1024 + x * 256, 256), 256)], tab.at[i], local_sems.at[7 + i]
            )
        )
    for copy in local:
        copy.start()

    moves = []

    def move(src, dst, peer, incoming):
        k = len(moves)
        moves.append(Move((send_sems.at[k], recv_sems.at[k]), src, dst, peer, incoming))
        return moves[-1]

    def ring(view):
        steps = {}
        for s in range(1, 4):
            up, down = view(z - s + 1), view(z + s - 1)
            steps[s] = (move(up, up, zp, view(z - s)), move(down, down, zm, view(z + s)))
        up, down = view(z - 3, 0), view(z + 3, 1)
        steps[4] = (move(up, up, zp, view(z - 4, 0)), move(down, down, zm, view(z + 4, 1)))
        return steps

    colour = m4(x + 2 * y)

    def quarter(ch, zo, q, part=None):
        columns = pl.ds(RANK * ch, RANK)
        if part is None:
            return wd.at[m8(zo), pl.ds(pl.multiple_of(m4(q) * 32, 32), 32), columns]
        return wd.at[m8(zo), pl.ds(pl.multiple_of(m4(q) * 32 + 16 * part, 16), 16), columns]

    def sides_of(ch, zo):
        own = quarter(ch, zo, colour)
        first, second = quarter(ch, zo, colour, 0), quarter(ch, zo, colour, 1)
        return (
            move(own, own, xp, quarter(ch, zo, colour - 1)),
            move(own, own, xm, quarter(ch, zo, colour + 1)),
            move(first, first, yp, quarter(ch, zo, colour + 2, 0)),
            move(second, second, ym, quarter(ch, zo, colour + 2, 1)),
        )

    down = [ring(functools.partial(lambda ch, zo, part=None: quarter(ch, zo, colour, part), ch)) for ch in range(2)]
    sides = [{d: sides_of(ch, z + d) for d in (-1, 1, -2, 2, -3, 3, 4)} for ch in range(2)]
    tokens_over = move(tk, pt, partner, pt)
    partial_over = [move(part_send.at[ch], part_recv.at[ch], partner, part_recv.at[ch]) for ch in range(2)]

    def up_block(zo, part=None, core=c):
        if part is None:
            return wup.at[m8(zo) * 2 + core]
        return wup.at[m8(zo) * 2 + core, pl.ds(16 * part, 16)]

    up = ring(up_block)
    up_hand = {
        d: move(up_block(z + d), up_block(z + d), partner, up_block(z + d, core=1 - c))
        for d in (0, -1, 1, -2, 2, -3, 3, 4)
    }

    def out_view(chunk, zo, part=None):
        lo, size = (512 * chunk, 512) if part is None else (512 * chunk + 256 * part, 256)
        return wo.at[pl.ds(lo, size), pl.ds(pl.multiple_of(m8(zo) * 256 + c * 128, 128), 128)]

    def out_column(zo, core):
        return wo.at[:, pl.ds(pl.multiple_of(m8(zo) * 256 + core * 128, 128), 128)]

    out = [ring(functools.partial(out_view, chunk)) for chunk in range(4)]
    out_hand = {
        d: move(out_column(z + d, c), out_column(z + d, c), partner, out_column(z + d, 1 - c))
        for d in (0, -1, 1, -2, 2, -3, 3, 4)
    }

    def hand(hands, step):
        for d in (-step, step) if step < 4 else (4,):
            hands[d].start()

    def out_visit(step, chunk):
        wait_all(out[chunk][step])
        if step < 4:
            start_all(out[chunk][step + 1])
        if chunk == 3:
            hand(out_hand, step)

    mid_a, mid_b = A_ROWS // 2, A_ROWS + (KV_ROWS - A_ROWS) // 2

    def rows_of(spans, oy, ox, part=None):
        lo, hi = spans[0 if part is None else part + 1]
        return kvb.at[m4(oy) * 4 + m4(ox), pl.ds(lo, hi - lo)]

    a_piece = functools.partial(rows_of, ((0, A_ROWS), (0, mid_a), (mid_a, A_ROWS)))
    b_piece = functools.partial(rows_of, ((A_ROWS, KV_ROWS), (A_ROWS, mid_b), (mid_b, KV_ROWS)))

    def q_piece(oy, ox, part=None):
        if part is None:
            return qb.at[m4(oy)]
        return qb.at[m4(oy), pl.ds(128 * part, 128)]

    def x_first(piece, oy):
        own = piece(oy, x)
        return move(own, own, xp, piece(oy, x - 1)), move(own, own, xm, piece(oy, x + 1))

    def x_second(piece, oy):
        left, right = piece(oy, x - 1, 0), piece(oy, x + 1, 1)
        return move(left, left, xp, piece(oy, x - 2, 0)), move(right, right, xm, piece(oy, x + 2, 1))

    def y_first(piece, ox):
        own = piece(y, ox)
        return move(own, own, yp, piece(y - 1, ox)), move(own, own, ym, piece(y + 1, ox))

    def y_second(piece, ox):
        under, over = piece(y - 1, ox, 0), piece(y + 1, ox, 1)
        return move(under, under, yp, piece(y - 2, ox, 0)), move(over, over, ym, piece(y + 2, ox, 1))

    ax1, ax2 = x_first(a_piece, y), x_second(a_piece, y)
    ay1 = {d: y_first(a_piece, x + d) for d in (0, -1, 1, 2)}
    ay2 = {d: y_second(a_piece, x + d) for d in (0, -1, 1, 2)}
    by1, by2 = y_first(b_piece, x), y_second(b_piece, x)
    bx1 = {d: x_first(b_piece, y + d) for d in (0, -1, 1, 2)}
    bx2 = {d: x_second(b_piece, y + d) for d in (0, -1, 1, 2)}
    qy1, qy2 = y_first(q_piece, x), y_second(q_piece, x)
    back = {
        d: move(osend.at[m4(y + d)], orecv.at[y], plane(y + d, x), orecv.at[m4(y - d)]) for d in (2, 1, 3)
    }

    barrier = pltpu.get_barrier_semaphore()
    for peer in (xp, xm, yp, ym, plane(y + 2, x), zp, zm, partner):
        pl.semaphore_signal(barrier, inc=1, device_id=peer, device_id_type=MESH)
    pl.semaphore_wait(barrier, 8)

    local[0].wait()
    start_all(down[0][1])
    local[1].wait()
    start_all(down[1][1])
    local[2].wait()
    tokens_over.start()

    local[3].wait()
    for h in range(4):
        wup[dp, :, NOPE * h : NOPE * (h + 1)] = wqs[:, 192 * h : 192 * h + NOPE]
    wup[dp, :, Q_WIDTH : Q_WIDTH + R_WIDTH] = jnp.concatenate(
        [wqs[:, 192 * h + NOPE : 192 * (h + 1)] for h in range(4)], axis=1
    )
    local[4].wait()
    start_all(up[1])
    up_hand[0].start()

    for copy in local[6:11]:
        copy.wait()
    own_tab = tab[y]
    kr = lax.dot_general(tk[...], wrot[...], (((1,), (1,)), ((), ())), preferred_element_type=F32)
    kr_swap = jnp.concatenate([kr[:, 32:], kr[:, :32]], axis=1)
    kr = (kr * own_tab[:, :64] + kr_swap * own_tab[:, 64:]).astype(BF16)
    packed = jnp.concatenate([kr[:128], kr[128:]], axis=1)
    for t in range(4):
        kvb[sp, BLOCK:KV_ROWS, 128 * t : 128 * (t + 1)] = packed[32 * t : 32 * (t + 1)]

    for step in range(1, 5):
        for ch in range(2):
            wait_all(down[ch][step])
            if step < 4:
                start_all(down[ch][step + 1])
            for d in (-step, step) if step < 4 else (4,):
                start_all(sides[ch][d])
        if step == 1:
            tokens_over.wait()
            for zo in range(8):
                columns = pl.ds(pl.multiple_of(256 * zo + 128 * c, 128), 128)
                lhs[0:256, 128 * zo : 128 * (zo + 1)] = tk[:, columns]
                lhs[256:512, 128 * zo : 128 * (zo + 1)] = pt[:, columns]
        else:
            wait_all(up[step - 1])
            start_all(up[step])
            hand(up_hand, step - 1)
        if step == 2:
            acc[...] = jnp.zeros_like(acc)
            mbuf[...] = jnp.full_like(mbuf, -jnp.inf)
        if step == 3:
            for h in range(4):
                vbuf[h, :, :, VDIM:256] = jnp.ones((16, BLOCK, 256 - VDIM), BF16)

    local[5].wait()
    for chunk in range(4):
        start_all(out[chunk][1])

    def down_project(ch):
        for d in (-1, 1, -2, 2, -3, 3, 4):
            wait_all(sides[ch][d])
        weights = wd[:, :, RANK * ch : RANK * (ch + 1)].reshape(1024, RANK)
        part_send[ch] = dot(lhs[256:512], weights)
        partial_over[ch].start()
        own = dot(lhs[0:256], weights)
        partial_over[ch].wait()
        return own + part_recv[ch]

    kvb[sp, 0:BLOCK, :] = norm(down_project(0), kv_gain[...]).astype(BF16)
    start_all(ax1 + bx1[0] + by1 + ay1[0])
    qb[y] = norm(down_project(1), q_gain[...]).astype(BF16)
    start_all(qy1)
    wait_all(up[4])
    hand(up_hand, 4)

    def expand_queries(i):
        rows = dot(qb[i], wup[:, :, 0 : Q_WIDTH + R_WIDTH].reshape(RANK, Q_WIDTH + R_WIDTH))
        first_half = lax.rem(lax.broadcasted_iota(jnp.int32, (BLOCK, R_WIDTH), 1), 64) < 32
        low = lax.broadcasted_iota(jnp.int32, (BLOCK, 128), 1) < 64
        table = tab[i]
        cosine = jnp.concatenate([table[:, :64]] * 4, axis=1)
        sine = jnp.concatenate([table[:, 64:]] * 4, axis=1)
        u = rows[:, Q_WIDTH:]
        swapped = jnp.where(first_half, pltpu.roll(u, R_WIDTH - 32, 1), pltpu.roll(u, 32, 1))
        turned = u * cosine + swapped * sine
        for h in range(4):
            qcat[h, i, :, 0:NOPE] = rows[:, NOPE * h : NOPE * (h + 1)].astype(BF16)
            pair = turned[:, 128 * (h // 2) : 128 * (h // 2 + 1)]
            keep = low if h % 2 == 0 else jnp.logical_not(low)
            qcat[h, i, :, NOPE:256] = jnp.where(keep, pair, 0.0).astype(BF16)

    def expand_keys(oy, ox):
        o = m4(oy) * 4 + m4(ox)
        rows = dot(kvb[o, 0:BLOCK, :], wup[:, :, Q_WIDTH + R_WIDTH :].reshape(RANK, 1024)).astype(BF16)
        low = lax.broadcasted_iota(jnp.int32, (32, 128), 1) < 64
        for h in range(4):
            kcat[h, o, :, 0:NOPE] = rows[:, 256 * h : 256 * h + NOPE]
            vbuf[h, o, :, 0:VDIM] = rows[:, 256 * h + NOPE : 256 * (h + 1)]
        for t in range(4):
            pair = kvb[o, BLOCK:KV_ROWS, 128 * t : 128 * (t + 1)].astype(F32)
            turned = pltpu.roll(pair, 64, 1)
            first = jnp.where(low, pair, turned).astype(BF16)
            second = jnp.where(low, turned, pair).astype(BF16)
            for h in range(4):
                kcat[h, o, 32 * t : 32 * (t + 1), NOPE:256] = first
                kcat[h, o, 128 + 32 * t : 128 + 32 * (t + 1), NOPE:256] = second

    def expand_many(which):
        dy, dxs = which

        def step(j, carry):
            expand_keys(y + dy, x + dxs[0] + j * (dxs[-1] - dxs[0]))
            return carry

        lax.fori_loop(0, len(dxs), step, 0)

    wait_all(ax1)
    start_all(ax2 + ay1[-1] + ay1[1])
    wait_all(bx1[0])
    start_all(bx2[0])
    wait_all(by1)
    start_all(by2 + bx1[1] + bx1[-1])
    wait_all(up_hand.values())
    expand_many((0, (0,)))
    expand_queries(y)
    wait_all(ay1[0])
    start_all(ay2[0])
    wait_all(ax2)
    start_all(ay1[2])
    out_visit(1, 0)
    expand_many((0, (-1, 1)))
    wait_all(qy1)
    start_all(qy2)
    out_visit(1, 1)

    def near_queries(j, carry):
        expand_queries(m4(y - 1 + 2 * j))
        return carry

    lax.fori_loop(0, 2, near_queries, 0)
    wait_all(by2)
    start_all(bx1[2])
    wait_all(bx2[0])
    expand_many((0, (2,)))
    out_visit(1, 2)

    def attend(i, r, masked):
        def scores_of(h):
            k = kcat[h, pl.ds(4 * r, 4)].reshape(1024, 256)
            return lax.dot_general(qcat[h, i], k, (((1,), (1,)), ((), ())), preferred_element_type=F32)

        def take(h, s):
            if masked:
                q_pos = lax.broadcasted_iota(jnp.int32, (256, 1024), 0) + x * 256
                k_pos = lax.broadcasted_iota(jnp.int32, (256, 1024), 1)
                s = jnp.where(k_pos <= q_pos, s, -jnp.inf)
            old = mbuf[h, i]
            top = jnp.maximum(old, jnp.max(s, axis=-1, keepdims=True) * SCALE)
            p = jnp.exp2(s * SCALE - top[:, :1]).astype(BF16)
            alpha = jnp.exp2(old - top)
            mbuf[h, i] = top
            v = vbuf[h, pl.ds(4 * r, 4)].reshape(1024, 256)
            acc[h, i] = acc[h, i] * jnp.concatenate([alpha, alpha], axis=1) + dot(p, v)

        ahead = scores_of(0)
        for h in range(4):
            s, ahead = ahead, scores_of(h + 1) if h < 3 else None
            take(h, s)

    def finish(i):
        for h in range(4):
            done = acc[h, i]
            osend[i, :, VDIM * h : VDIM * (h + 1)] = (done[:, :VDIM] / done[:, VDIM:]).astype(BF16)

    def at_1():
        wait_all(ay1[-1])
        start_all(ay2[-1])
        wait_all(ay1[1])
        start_all(ay2[1])

    def at_2():
        wait_all(bx1[1])
        start_all(bx2[1])
        wait_all(bx1[-1])
        start_all(bx2[-1])

    def at_3():
        wait_all(qy2)
        expand_queries(m4(y + 2))

    def at_4():
        wait_all(ay1[2])
        start_all(ay2[2])
        expand_many((1, (0,)))
        expand_many((1, (-1, 1)))
        wait_all(bx2[1])
        expand_many((1, (2,)))

    def at_6():
        wait_all(bx1[2])
        start_all(bx2[2])

    def at_8():
        expand_many((-1, (0,)))
        expand_many((-1, (-1, 1)))
        wait_all(bx2[-1])
        expand_many((-1, (2,)))

    def at_12():
        wait_all(ay2[0])
        expand_many((2, (0,)))
        wait_all(ay2[-1] + ay2[1])
        expand_many((2, (-1, 1)))
        wait_all(ay2[2] + bx2[2])
        expand_many((2, (2,)))

    events = {1: at_1, 2: at_2, 3: at_3, 4: at_4, 6: at_6, 8: at_8, 12: at_12}
    visits = {0: (1, 3), 1: (2, 0), 2: (2, 1), 3: (2, 2), 4: (2, 3), 6: (3, 0), 7: (3, 1), 8: (3, 2), 9: (3, 3)}

    def slot(v, done):
        rho, kappa = lax.div(v, 4), lax.rem(v, 4)
        swap = jnp.where(kappa == 2, 3, jnp.where(kappa == 3, 2, kappa))
        dr = jnp.where(rho == 2, 3, jnp.where(rho == 3, 2, rho))
        last = jnp.where(kappa == 0, 2, jnp.where(kappa == 2, 3, jnp.where(kappa == 3, 0, 1)))
        r, i = m4(y + dr), m4(y + jnp.where(rho == 3, last, swap))
        for at, event in events.items():
            pl.when(v == at)(event)
        pl.when(i == r)(lambda: attend(i, r, True))
        pl.when(i > r)(lambda: attend(i, r, False))
        active = i >= r
        for number, (step, chunk) in visits.items():
            pl.when(jnp.logical_and(active, done == number))(functools.partial(out_visit, step, chunk))
        pl.when(rho == 3)(lambda: finish(i))
        for at, d in ((12, 2), (13, 1), (14, 3)):
            pl.when(v == at)(back[d].start)
        return done + active.astype(jnp.int32)

    lax.fori_loop(0, 16, slot, jnp.int32(0))

    out_hand[0].start()
    for chunk in range(4):
        out_visit(4, chunk)
    wait_all(out_hand.values())

    def project(attended, j):
        return dot(attended, wo[pl.ds(pl.multiple_of(512 * j, 512), 512), :])

    total = project(osend[y], y)
    for d in (3, 1, 2):
        back[d].wait()
        total = total + project(orecv[m4(y - d)], m4(y - d))
    out_ref[...] = norm(total, out_gain[...]).astype(BF16)
    for each in moves:
        each.finish()


N_COPIES = 208


def body(tokens, w_qdown, w_kvdown, w_rotary, q_gain, kv_gain, w_qup, w_kvup, w_out, out_gain):
    table = jnp.asarray(turn_table())
    any_spec = pl.BlockSpec(memory_space=pl.ANY)
    vmem_spec = pl.BlockSpec(memory_space=pltpu.VMEM)
    call = pl.pallas_call(
        kernel,
        out_shape=jax.ShapeDtypeStruct((BLOCK, D), BF16),
        in_specs=[any_spec, any_spec, any_spec, any_spec, vmem_spec, vmem_spec]
        + [any_spec, any_spec, any_spec, vmem_spec, any_spec],
        out_specs=vmem_spec,
        scratch_shapes=[
            pltpu.VMEM((BLOCK, D), BF16),
            pltpu.VMEM((BLOCK, D), BF16),
            pltpu.VMEM((2 * BLOCK, 1024), BF16),
            pltpu.VMEM((8, 128, 1024), BF16),
            pltpu.VMEM((2, BLOCK, RANK), F32),
            pltpu.VMEM((2, BLOCK, RANK), F32),
            pltpu.VMEM((16, KV_ROWS, RANK), BF16),
            pltpu.VMEM((4, BLOCK, RANK), BF16),
            pltpu.VMEM((32, 768), BF16),
            pltpu.VMEM((16, 32, UP_WIDTH), BF16),
            pltpu.VMEM((D, D), BF16),
            pltpu.VMEM((ROPE, D), BF16),
            pltpu.VMEM((4, BLOCK, 128), F32),
            pltpu.VMEM((4, 16, BLOCK, 256), BF16),
            pltpu.VMEM((4, 16, BLOCK, 256), BF16),
            pltpu.VMEM((4, 4, BLOCK, 256), BF16),
            pltpu.VMEM((4, 4, BLOCK, 256), F32),
            pltpu.VMEM((4, 4, BLOCK, 128), F32),
            pltpu.VMEM((4, BLOCK, 512), BF16),
            pltpu.VMEM((4, BLOCK, 512), BF16),
            pltpu.SemaphoreType.DMA((N_COPIES,)),
            pltpu.SemaphoreType.DMA((N_COPIES,)),
            pltpu.SemaphoreType.DMA((11,)),
        ],
        compiler_params=pltpu.CompilerParams(
            collective_id=0, has_side_effects=True, vmem_limit_bytes=63 * 1024 * 1024
        ),
        name="latent_attention",
    )
    mixed = call(
        tokens[0], w_qdown, w_kvdown, w_rotary.T, q_gain[None], kv_gain[None],
        w_qup, w_kvup, w_out, out_gain[None], table,
    )
    return mixed[None]


def solution(mesh):
    in_specs = (
        P("dp", "sp", None),
        P("dp", None),
        P("dp", None),
        P(),
        P(),
        P(),
        P("dp", None),
        P("dp", None),
        P(None, "dp"),
        P(),
    )
    out_specs = P("dp", "sp", None)
    return jax.shard_map(body, mesh=mesh, in_specs=in_specs, out_specs=out_specs, check_vma=False)
```

```python
import functools

import jax
import jax.numpy as jnp
import numpy as np
from jax import lax
from jax.experimental import pallas as pl
from jax.experimental.pallas import tpu as pltpu
from jax.sharding import PartitionSpec as P

HEADS = 16
NOPE = 128
ROPE = 64
VDIM = 128
D = 2048
RANK = 512
LENGTH = 4096
BLOCK = 256
EPSILON = 1e-06
THETA = 10000.0
LOG2E = 1.4426950408889634
SCALE = (NOPE + ROPE) ** (-0.5) * LOG2E
MESH = pl.DeviceIdType.MESH
BF16 = jnp.bfloat16
F32 = jnp.float32
Q_WIDTH = 4 * NOPE
R_WIDTH = 4 * ROPE
UP_WIDTH = Q_WIDTH + R_WIDTH + 4 * (NOPE + VDIM)
A_ROWS = 96
PLACE = {0: 0, -1: 1, 1: 2, 2: 3}
KEY_BLOCKS = 4
SUBS = 4 // KEY_BLOCKS
KV_ROWS = BLOCK + 32


def turn_table():
    positions = np.arange(LENGTH).astype(np.float32)
    freqs = np.float32(THETA) ** (-np.arange(0, ROPE, 2).astype(np.float32) / np.float32(ROPE))
    angles = positions[:, None] * freqs[None, :].astype(np.float32)
    cosine, sine = np.cos(angles), np.sin(angles)
    return np.concatenate([cosine, cosine, -sine, sine], axis=1).astype(np.float32)


def dot(a, b):
    return jnp.dot(a, b, preferred_element_type=F32)


class Move:
    def __init__(self, sems, src, dst, peer, incoming):
        def make(a, b):
            return pltpu.make_async_remote_copy(
                src_ref=a, dst_ref=b, send_sem=sems[0], recv_sem=sems[1], device_id=peer, device_id_type=MESH
            )

        self.out, self.into = make(src, dst), make(incoming, incoming)

    def start(self):
        self.out.start()

    def wait(self):
        self.into.wait_recv()

    def finish(self):
        self.out.wait_send()


def start_all(moves):
    for move in moves:
        move.start()


def wait_all(moves):
    for move in moves:
        move.wait()


def norm(v, gain):
    return v * lax.rsqrt(jnp.mean(v * v, axis=-1, keepdims=True) + EPSILON) * gain


def kernel(
    tok_hbm, wq_hbm, wkv_hbm, wrot_hbm, q_gain, kv_gain, wqup_hbm, wkvup_hbm, wout_hbm, out_gain, tab_hbm,
    out_ref,
    tk, pt, lhs, wd, part_send, part_recv, kvb, qb, wqs, wup, wo, wrot, tab, kcat, vbuf, qcat, acc, mbuf,
    osend, orecv, send_sems, recv_sems, local_sems,
):
    sp, dp = lax.axis_index("sp"), lax.axis_index("dp")
    y, x = lax.div(sp, 4), lax.rem(sp, 4)
    z, c = lax.div(dp, 2), lax.rem(dp, 2)

    def m4(v):
        return lax.rem(v + 8, 4)

    def m8(v):
        return lax.rem(v + 16, 8)

    def plane(yy, xx):
        return (m4(yy) * 4 + m4(xx), dp)

    def along(zz):
        return (sp, m8(zz) * 2 + c)

    partner = (sp, z * 2 + (1 - c))
    xp, xm, yp, ym = plane(y, x + 1), plane(y, x - 1), plane(y + 1, x), plane(y - 1, x)
    zp, zm = along(z + 1), along(z - 1)

    local = [
        pltpu.make_async_copy(wkv_hbm, wd.at[z, :, pl.ds(0, RANK)], local_sems.at[0]),
        pltpu.make_async_copy(wq_hbm, wd.at[z, :, pl.ds(RANK, RANK)], local_sems.at[1]),
        pltpu.make_async_copy(tok_hbm, tk, local_sems.at[2]),
        pltpu.make_async_copy(
            wqup_hbm.at[:, pl.ds(pl.multiple_of(y * 768, 128), 768)], wqs, local_sems.at[3]
        ),
        pltpu.make_async_copy(
            wkvup_hbm.at[:, pl.ds(pl.multiple_of(y * 1024, 128), 1024)],
            wup.at[dp, :, pl.ds(Q_WIDTH + R_WIDTH, 1024)],
            local_sems.at[4],
        ),
        pltpu.make_async_copy(
            wout_hbm, wo.at[:, pl.ds(pl.multiple_of(dp * 128, 128), 128)], local_sems.at[5]
        ),
        pltpu.make_async_copy(wrot_hbm, wrot, local_sems.at[6]),
    ]
    for i in range(4):
        local.append(
            pltpu.make_async_copy(
                tab_hbm.at[pl.ds(pl.multiple_of(i * 1024 + x * 256, 256), 256)], tab.at[i], local_sems.at[7 + i]
            )
        )
    for copy in local:
        copy.start()

    moves = []

    def move(src, dst, peer, incoming):
        k = len(moves)
        moves.append(Move((send_sems.at[k], recv_sems.at[k]), src, dst, peer, incoming))
        return moves[-1]

    def ring(view):
        steps = {}
        for s in range(1, 4):
            up, down = view(z - s + 1), view(z + s - 1)
            steps[s] = (move(up, up, zp, view(z - s)), move(down, down, zm, view(z + s)))
        up, down = view(z - 3, 0), view(z + 3, 1)
        steps[4] = (move(up, up, zp, view(z - 4, 0)), move(down, down, zm, view(z + 4, 1)))
        return steps

    colour = m4(x + 2 * y)

    def quarter(ch, zo, q, part=None):
        columns = pl.ds(RANK * ch, RANK)
        if part is None:
            return wd.at[m8(zo), pl.ds(pl.multiple_of(m4(q) * 32, 32), 32), columns]
        return wd.at[m8(zo), pl.ds(pl.multiple_of(m4(q) * 32 + 16 * part, 16), 16), columns]

    def sides_of(ch, zo):
        own = quarter(ch, zo, colour)
        first, second = quarter(ch, zo, colour, 0), quarter(ch, zo, colour, 1)
        return (
            move(own, own, xp, quarter(ch, zo, colour - 1)),
            move(own, own, xm, quarter(ch, zo, colour + 1)),
            move(first, first, yp, quarter(ch, zo, colour + 2, 0)),
            move(second, second, ym, quarter(ch, zo, colour + 2, 1)),
        )

    near = (-1, 1, -2, 2, -3, 3, 4)
    own_quarter = quarter(0, z, colour)
    direct = {d: move(own_quarter, own_quarter, along(z + d), quarter(0, z - d, colour)) for d in near}
    down = ring(lambda zo, part=None: quarter(1, zo, colour, part))
    sides = [{d: sides_of(ch, z + d) for d in near} for ch in range(2)]
    tokens_over = move(tk, pt, partner, pt)
    partial_over = [move(part_send.at[ch], part_recv.at[ch], partner, part_recv.at[ch]) for ch in range(2)]

    def up_block(zo, part=None, core=c):
        if part is None:
            return wup.at[m8(zo) * 2 + core]
        return wup.at[m8(zo) * 2 + core, pl.ds(16 * part, 16)]

    up = ring(up_block)
    up_hand = {
        d: move(up_block(z + d), up_block(z + d), partner, up_block(z + d, core=1 - c))
        for d in (0, -1, 1, -2, 2, -3, 3, 4)
    }

    def out_view(chunk, zo, part=None):
        lo, size = (512 * chunk, 512) if part is None else (512 * chunk + 256 * part, 256)
        return wo.at[pl.ds(lo, size), pl.ds(pl.multiple_of(m8(zo) * 256 + c * 128, 128), 128)]

    def out_column(zo, core):
        return wo.at[:, pl.ds(pl.multiple_of(m8(zo) * 256 + core * 128, 128), 128)]

    out = [ring(functools.partial(out_view, chunk)) for chunk in range(4)]
    out_hand = {
        d: move(out_column(z + d, c), out_column(z + d, c), partner, out_column(z + d, 1 - c))
        for d in (0, -1, 1, -2, 2, -3, 3, 4)
    }

    def hand(hands, step):
        for d in (-step, step) if step < 4 else (4,):
            hands[d].start()

    def out_visit(step, chunk):
        wait_all(out[chunk][step])
        if step < 4:
            start_all(out[chunk][step + 1])
        if chunk == 3:
            hand(out_hand, step)

    mid_a, mid_b = A_ROWS // 2, A_ROWS + (KV_ROWS - A_ROWS) // 2

    def rows_of(spans, oy, ox, part=None):
        lo, hi = spans[0 if part is None else part + 1]
        return kvb.at[m4(oy) * 4 + m4(ox), pl.ds(lo, hi - lo)]

    a_piece = functools.partial(rows_of, ((0, A_ROWS), (0, mid_a), (mid_a, A_ROWS)))
    b_piece = functools.partial(rows_of, ((A_ROWS, KV_ROWS), (A_ROWS, mid_b), (mid_b, KV_ROWS)))

    def q_piece(oy, ox, part=None):
        if part is None:
            return qb.at[m4(oy)]
        return qb.at[m4(oy), pl.ds(128 * part, 128)]

    def x_first(piece, oy):
        own = piece(oy, x)
        return move(own, own, xp, piece(oy, x - 1)), move(own, own, xm, piece(oy, x + 1))

    def x_second(piece, oy):
        left, right = piece(oy, x - 1, 0), piece(oy, x + 1, 1)
        return move(left, left, xp, piece(oy, x - 2, 0)), move(right, right, xm, piece(oy, x + 2, 1))

    def y_first(piece, ox):
        own = piece(y, ox)
        return move(own, own, yp, piece(y - 1, ox)), move(own, own, ym, piece(y + 1, ox))

    def y_second(piece, ox):
        under, over = piece(y - 1, ox, 0), piece(y + 1, ox, 1)
        return move(under, under, yp, piece(y - 2, ox, 0)), move(over, over, ym, piece(y + 2, ox, 1))

    ax1, ax2 = x_first(a_piece, y), x_second(a_piece, y)
    ay1 = {d: y_first(a_piece, x + d) for d in (0, -1, 1, 2)}
    ay2 = {d: y_second(a_piece, x + d) for d in (0, -1, 1, 2)}
    by1, by2 = y_first(b_piece, x), y_second(b_piece, x)
    bx1 = {d: x_first(b_piece, y + d) for d in (0, -1, 1, 2)}
    bx2 = {d: x_second(b_piece, y + d) for d in (0, -1, 1, 2)}
    qy1, qy2 = y_first(q_piece, x), y_second(q_piece, x)
    back = {
        d: move(osend.at[m4(y + d)], orecv.at[y], plane(y + d, x), orecv.at[m4(y - d)]) for d in (2, 1, 3)
    }

    barrier = pltpu.get_barrier_semaphore()
    for peer in (xp, xm, yp, ym, plane(y + 2, x), partner) + tuple(along(z + d) for d in near):
        pl.semaphore_signal(barrier, inc=1, device_id=peer, device_id_type=MESH)
    pl.semaphore_wait(barrier, 13)

    local[0].wait()
    for d in (4, -3, 3, -2, 2, -1, 1):
        direct[d].start()
    local[2].wait()
    tokens_over.start()
    local[1].wait()
    start_all(down[1])

    local[3].wait()
    for h in range(4):
        wup[dp, :, NOPE * h : NOPE * (h + 1)] = wqs[:, 192 * h : 192 * h + NOPE]
    wup[dp, :, Q_WIDTH : Q_WIDTH + R_WIDTH] = jnp.concatenate(
        [wqs[:, 192 * h + NOPE : 192 * (h + 1)] for h in range(4)], axis=1
    )
    local[4].wait()
    start_all(up[1])
    up_hand[0].start()

    def relay(step):
        wait_all(down[step] + up[step])
        if step < 4:
            start_all(down[step + 1] + up[step + 1])
        for d in (-step, step) if step < 4 else (4,):
            start_all(sides[1][d])
        hand(up_hand, step)

    def pass_on(d):
        direct[-d if d != 4 else 4].wait()
        start_all(sides[0][d])

    for copy in local[6:11]:
        copy.wait()
    own_tab = tab[y]
    kr = lax.dot_general(tk[...], wrot[...], (((1,), (1,)), ((), ())), preferred_element_type=F32)
    kr_swap = jnp.concatenate([kr[:, 32:], kr[:, :32]], axis=1)
    kr = (kr * own_tab[:, :64] + kr_swap * own_tab[:, 64:]).astype(BF16)
    packed = jnp.concatenate([kr[:128], kr[128:]], axis=1)
    for t in range(4):
        kvb[sp, BLOCK:KV_ROWS, 128 * t : 128 * (t + 1)] = packed[32 * t : 32 * (t + 1)]

    for d in (-1, 1, -2, 2):
        pass_on(d)
    tokens_over.wait()
    for zo in range(8):
        columns = pl.ds(pl.multiple_of(256 * zo + 128 * c, 128), 128)
        lhs[0:256, 128 * zo : 128 * (zo + 1)] = tk[:, columns]
        lhs[256:512, 128 * zo : 128 * (zo + 1)] = pt[:, columns]
    for d in (-3, 3, 4):
        pass_on(d)
    relay(1)
    for h in range(4):
        vbuf[h, :, :, VDIM:256] = jnp.ones((16, BLOCK, 256 - VDIM), BF16)
    relay(2)
    acc[...] = jnp.zeros_like(acc)
    mbuf[...] = jnp.full_like(mbuf, -jnp.inf)

    def down_project(ch):
        for d in near:
            wait_all(sides[ch][d])
        weights = wd[:, :, RANK * ch : RANK * (ch + 1)].reshape(1024, RANK)
        part_send[ch] = dot(lhs[256:512], weights)
        partial_over[ch].start()
        own = dot(lhs[0:256], weights)
        partial_over[ch].wait()
        return own + part_recv[ch]

    kvb[sp, 0:BLOCK, :] = norm(down_project(0), kv_gain[...]).astype(BF16)
    start_all(ax1 + bx1[0] + by1 + ay1[0])
    relay(3)
    relay(4)
    local[5].wait()
    for chunk in range(4):
        start_all(out[chunk][1])
    wait_all(ax1)
    start_all(ax2 + ay1[-1] + ay1[1])
    wait_all(bx1[0])
    start_all(bx2[0])
    wait_all(by1)
    start_all(by2 + bx1[1] + bx1[-1])
    qb[y] = norm(down_project(1), q_gain[...]).astype(BF16)
    start_all(qy1)

    def expand_queries(i):
        rows = dot(qb[i], wup[:, :, 0 : Q_WIDTH + R_WIDTH].reshape(RANK, Q_WIDTH + R_WIDTH))
        first_half = lax.rem(lax.broadcasted_iota(jnp.int32, (BLOCK, R_WIDTH), 1), 64) < 32
        low = lax.broadcasted_iota(jnp.int32, (BLOCK, 128), 1) < 64
        table = tab[i]
        cosine = jnp.concatenate([table[:, :64]] * 4, axis=1)
        sine = jnp.concatenate([table[:, 64:]] * 4, axis=1)
        u = rows[:, Q_WIDTH:]
        swapped = jnp.where(first_half, pltpu.roll(u, R_WIDTH - 32, 1), pltpu.roll(u, 32, 1))
        turned = u * cosine + swapped * sine
        for h in range(4):
            qcat[h, i, :, 0:NOPE] = rows[:, NOPE * h : NOPE * (h + 1)].astype(BF16)
            pair = turned[:, 128 * (h // 2) : 128 * (h // 2 + 1)]
            keep = low if h % 2 == 0 else jnp.logical_not(low)
            qcat[h, i, :, NOPE:256] = jnp.where(keep, pair, 0.0).astype(BF16)

    def expand_keys(oy, ox, place):
        source, o = m4(oy) * 4 + m4(ox), m4(oy) * 4 + place
        rows = dot(kvb[source, 0:BLOCK, :], wup[:, :, Q_WIDTH + R_WIDTH :].reshape(RANK, 1024)).astype(BF16)
        low = lax.broadcasted_iota(jnp.int32, (32, 128), 1) < 64
        for h in range(4):
            kcat[h, o, :, 0:NOPE] = rows[:, 256 * h : 256 * h + NOPE]
            vbuf[h, o, :, 0:VDIM] = rows[:, 256 * h + NOPE : 256 * (h + 1)]
        for t in range(4):
            pair = kvb[source, BLOCK:KV_ROWS, 128 * t : 128 * (t + 1)].astype(F32)
            turned = pltpu.roll(pair, 64, 1)
            first = jnp.where(low, pair, turned).astype(BF16)
            second = jnp.where(low, turned, pair).astype(BF16)
            for h in range(4):
                kcat[h, o, 32 * t : 32 * (t + 1), NOPE:256] = first
                kcat[h, o, 128 + 32 * t : 128 + 32 * (t + 1), NOPE:256] = second

    def expand_many(which):
        dy, dxs = which

        def step(j, carry):
            expand_keys(y + dy, x + dxs[0] + j * (dxs[-1] - dxs[0]), PLACE[dxs[0]] + j)
            return carry

        lax.fori_loop(0, len(dxs), step, 0)

    wait_all(up_hand.values())
    expand_many((0, (0,)))
    expand_queries(y)
    wait_all(ay1[0])
    start_all(ay2[0])
    wait_all(ax2)
    start_all(ay1[2])
    out_visit(1, 0)
    expand_many((0, (-1, 1)))
    wait_all(qy1)
    start_all(qy2)
    out_visit(1, 1)

    def near_queries(j, carry):
        expand_queries(m4(y - 1 + 2 * j))
        return carry

    lax.fori_loop(0, 2, near_queries, 0)
    wait_all(by2)
    start_all(bx1[2])
    wait_all(bx2[0])
    expand_many((0, (2,)))
    out_visit(1, 2)

    width = BLOCK * KEY_BLOCKS

    def column_of(place):
        return m4(x + jnp.where(place == 1, 3, jnp.where(place == 2, 1, jnp.where(place == 3, 2, 0))))

    def attend(i, r, sub, masked):
        first = 4 * r + KEY_BLOCKS * sub

        def scores_of(h):
            k = kcat[h, pl.ds(first, KEY_BLOCKS)].reshape(width, 256)
            return lax.dot_general(qcat[h, i], k, (((1,), (1,)), ((), ())), preferred_element_type=F32)

        def take(h, s):
            if masked:
                ahead = lax.broadcasted_iota(jnp.int32, (BLOCK, BLOCK), 1) - lax.broadcasted_iota(
                    jnp.int32, (BLOCK, BLOCK), 0
                )
                parts = []
                for b in range(KEY_BLOCKS):
                    limit = BLOCK * (x - column_of(KEY_BLOCKS * sub + b))
                    parts.append(jnp.where(ahead <= limit, s[:, BLOCK * b : BLOCK * (b + 1)], -jnp.inf))
                s = jnp.concatenate(parts, axis=1) if KEY_BLOCKS > 1 else parts[0]
            old = mbuf[h, i]
            top = jnp.maximum(old, jnp.max(s, axis=-1, keepdims=True) * SCALE)
            p = jnp.exp2(s * SCALE - top[:, :1]).astype(BF16)
            alpha = jnp.exp2(old - top)
            mbuf[h, i] = top
            v = vbuf[h, pl.ds(first, KEY_BLOCKS)].reshape(width, 256)
            acc[h, i] = acc[h, i] * jnp.concatenate([alpha, alpha], axis=1) + dot(p, v)

        ahead = scores_of(0)
        for h in range(4):
            s, ahead = ahead, scores_of(h + 1) if h < 3 else None
            take(h, s)

    def finish(i):
        for h in range(4):
            done = acc[h, i]
            osend[i, :, VDIM * h : VDIM * (h + 1)] = (done[:, :VDIM] / done[:, VDIM:]).astype(BF16)

    def at_1():
        wait_all(ay1[-1])
        start_all(ay2[-1])
        wait_all(ay1[1])
        start_all(ay2[1])

    def at_2():
        wait_all(bx1[1])
        start_all(bx2[1])
        wait_all(bx1[-1])
        start_all(bx2[-1])

    def at_3():
        wait_all(qy2)
        expand_queries(m4(y + 2))

    def at_4():
        wait_all(ay1[2])
        start_all(ay2[2])
        expand_many((1, (0,)))
        expand_many((1, (-1, 1)))
        wait_all(bx2[1])
        expand_many((1, (2,)))

    def at_6():
        wait_all(bx1[2])
        start_all(bx2[2])

    def at_8():
        expand_many((-1, (0,)))
        expand_many((-1, (-1, 1)))
        wait_all(bx2[-1])
        expand_many((-1, (2,)))

    def send_back(d):
        finish(m4(y + d))
        back[d].start()

    def at_last(place):
        if place == 0:
            for d in (1, 3):
                pl.when(m4(y + d) < m4(y + 2))(functools.partial(send_back, d))
            wait_all(ay2[0])
            expand_many((2, (0,)))
        elif place == 1:
            wait_all(ay2[-1])
            expand_many((2, (-1,)))
        elif place == 2:
            wait_all(ay2[1])
            expand_many((2, (1,)))
        else:
            wait_all(ay2[2] + bx2[2])
            expand_many((2, (2,)))

    def at_sub(sub):
        for b in range(KEY_BLOCKS):
            at_last(KEY_BLOCKS * sub + b)

    last_row = 12 * SUBS
    events = {1: at_1, 2: at_2, 3: at_3, 4: at_4, 6: at_6, 8: at_8}
    events = {SUBS * at: event for at, event in events.items()}
    events.update({last_row + 4 * sub: functools.partial(at_sub, sub) for sub in range(SUBS)})
    visits = {0: (1, 3), 1: (2, 0), 2: (2, 1), 3: (2, 2), 4: (2, 3), 6: (3, 0), 7: (3, 1), 8: (3, 2), 9: (3, 3)}

    def slot(v, done):
        late = v >= last_row
        rho = jnp.minimum(lax.div(v, 4 * SUBS), 3)
        kappa = jnp.where(late, lax.rem(v, 4), lax.rem(lax.div(v, SUBS), 4))
        sub = jnp.where(late, lax.div(v - last_row, 4), lax.rem(v, SUBS))
        swap = jnp.where(kappa == 2, 3, jnp.where(kappa == 3, 2, kappa))
        dr = jnp.where(rho == 2, 3, jnp.where(rho == 3, 2, rho))
        last = jnp.where(kappa == 0, 2, jnp.where(kappa == 2, 3, jnp.where(kappa == 3, 0, 1)))
        r, i = m4(y + dr), m4(y + jnp.where(late, last, swap))
        for at, event in events.items():
            pl.when(v == at)(event)
        if KEY_BLOCKS == 1:
            column = column_of(sub)
            edge = jnp.logical_and(i == r, column == x)
            whole = jnp.logical_or(i > r, jnp.logical_and(i == r, column < x))
        else:
            edge, whole = i == r, i > r
        pl.when(edge)(lambda: attend(i, r, sub, True))
        pl.when(whole)(lambda: attend(i, r, sub, False))
        active = i >= r
        for number, (step, chunk) in visits.items():
            pl.when(jnp.logical_and(active, done == SUBS * number))(functools.partial(out_visit, step, chunk))
        for at, d in ((0, 2), (1, 1), (2, 3)):
            pl.when(jnp.logical_and(v == last_row + 4 * (SUBS - 1) + at, active))(functools.partial(send_back, d))
        return done + active.astype(jnp.int32)

    lax.fori_loop(0, 16 * SUBS, slot, jnp.int32(0))
    finish(y)

    out_hand[0].start()
    for chunk in range(4):
        out_visit(4, chunk)
    wait_all(out_hand.values())

    def project(attended, j):
        return dot(attended, wo[pl.ds(pl.multiple_of(512 * j, 512), 512), :])

    total = project(osend[y], y)
    for d in (3, 1, 2):
        back[d].wait()
        total = total + project(orecv[m4(y - d)], m4(y - d))
    out_ref[...] = norm(total, out_gain[...]).astype(BF16)
    for each in moves:
        each.finish()


N_COPIES = 208


def body(tokens, w_qdown, w_kvdown, w_rotary, q_gain, kv_gain, w_qup, w_kvup, w_out, out_gain):
    table = jnp.asarray(turn_table())
    any_spec = pl.BlockSpec(memory_space=pl.ANY)
    vmem_spec = pl.BlockSpec(memory_space=pltpu.VMEM)
    call = pl.pallas_call(
        kernel,
        out_shape=pltpu.VMEM((BLOCK, D), BF16),
        in_specs=[any_spec, any_spec, any_spec, any_spec, vmem_spec, vmem_spec]
        + [any_spec, any_spec, any_spec, vmem_spec, any_spec],
        out_specs=vmem_spec,
        scratch_shapes=[
            pltpu.VMEM((BLOCK, D), BF16),
            pltpu.VMEM((BLOCK, D), BF16),
            pltpu.VMEM((2 * BLOCK, 1024), BF16),
            pltpu.VMEM((8, 128, 1024), BF16),
            pltpu.VMEM((2, BLOCK, RANK), F32),
            pltpu.VMEM((2, BLOCK, RANK), F32),
            pltpu.VMEM((16, KV_ROWS, RANK), BF16),
            pltpu.VMEM((4, BLOCK, RANK), BF16),
            pltpu.VMEM((32, 768), BF16),
            pltpu.VMEM((16, 32, UP_WIDTH), BF16),
            pltpu.VMEM((D, D), BF16),
            pltpu.VMEM((ROPE, D), BF16),
            pltpu.VMEM((4, BLOCK, 128), F32),
            pltpu.VMEM((4, 16, BLOCK, 256), BF16),
            pltpu.VMEM((4, 16, BLOCK, 256), BF16),
            pltpu.VMEM((4, 4, BLOCK, 256), BF16),
            pltpu.VMEM((4, 4, BLOCK, 256), F32),
            pltpu.VMEM((4, 4, BLOCK, 128), F32),
            pltpu.VMEM((4, BLOCK, 512), BF16),
            pltpu.VMEM((4, BLOCK, 512), BF16),
            pltpu.SemaphoreType.DMA((N_COPIES,)),
            pltpu.SemaphoreType.DMA((N_COPIES,)),
            pltpu.SemaphoreType.DMA((11,)),
        ],
        compiler_params=pltpu.CompilerParams(
            collective_id=0, has_side_effects=True, vmem_limit_bytes=58 * 1024 * 1024
        ),
        name="latent_attention",
    )
    mixed = call(
        tokens[0], w_qdown, w_kvdown, w_rotary.T, q_gain[None], kv_gain[None],
        w_qup, w_kvup, w_out, out_gain[None], table,
    )
    return mixed[None]


def solution(mesh):
    in_specs = (
        P("dp", "sp", None),
        P("dp", None),
        P("dp", None),
        P(),
        P(),
        P(),
        P("dp", None),
        P("dp", None),
        P(None, "dp"),
        P(),
    )
    out_specs = P("dp", "sp", None)
    return jax.shard_map(body, mesh=mesh, in_specs=in_specs, out_specs=out_specs, check_vma=False)
```

```python
import functools

import jax
import jax.numpy as jnp
import numpy as np
from jax import lax
from jax.experimental import pallas as pl
from jax.experimental.pallas import tpu as pltpu
from jax.sharding import PartitionSpec as P

HEADS = 16
NOPE = 128
ROPE = 64
VDIM = 128
D = 2048
RANK = 512
LENGTH = 4096
BLOCK = 256
EPSILON = 1e-06
THETA = 10000.0
LOG2E = 1.4426950408889634
SCALE = (NOPE + ROPE) ** (-0.5) * LOG2E
MESH = pl.DeviceIdType.MESH
BF16 = jnp.bfloat16
F32 = jnp.float32
Q_WIDTH = 4 * NOPE
R_WIDTH = 4 * ROPE
UP_WIDTH = Q_WIDTH + R_WIDTH + 4 * (NOPE + VDIM)
A_ROWS = 96
PLACE = {0: 0, -1: 1, 1: 2, 2: 3}
KEY_BLOCKS = 4
SUBS = 4 // KEY_BLOCKS
KV_ROWS = BLOCK + 32


def turn_table():
    positions = np.arange(LENGTH).astype(np.float32)
    freqs = np.float32(THETA) ** (-np.arange(0, ROPE, 2).astype(np.float32) / np.float32(ROPE))
    angles = positions[:, None] * freqs[None, :].astype(np.float32)
    cosine, sine = np.cos(angles), np.sin(angles)
    return np.concatenate([cosine, cosine, -sine, sine], axis=1).astype(np.float32)


def dot(a, b):
    return jnp.dot(a, b, preferred_element_type=F32)


class Move:
    def __init__(self, sems, src, dst, peer, incoming):
        def make(a, b):
            return pltpu.make_async_remote_copy(
                src_ref=a, dst_ref=b, send_sem=sems[0], recv_sem=sems[1], device_id=peer, device_id_type=MESH
            )

        self.out, self.into = make(src, dst), make(incoming, incoming)

    def start(self):
        self.out.start()

    def wait(self):
        self.into.wait_recv()

    def finish(self):
        self.out.wait_send()


def start_all(moves):
    for move in moves:
        move.start()


def wait_all(moves):
    for move in moves:
        move.wait()


def norm(v, gain):
    return v * lax.rsqrt(jnp.mean(v * v, axis=-1, keepdims=True) + EPSILON) * gain


def kernel(
    tok_hbm, wq_hbm, wkv_hbm, wrot_hbm, q_gain, kv_gain, wqup_hbm, wkvup_hbm, wout_hbm, out_gain, tab_hbm,
    out_ref,
    tk, pt, lhs, wd, part_send, part_recv, kvb, qb, wqs, wup, wo, wrot, tab, kcat, vbuf, qcat, acc, mbuf,
    osend, orecv, send_sems, recv_sems, local_sems,
):
    sp, dp = lax.axis_index("sp"), lax.axis_index("dp")
    y, x = lax.div(sp, 4), lax.rem(sp, 4)
    z, c = lax.div(dp, 2), lax.rem(dp, 2)

    def m4(v):
        return lax.rem(v + 8, 4)

    def m8(v):
        return lax.rem(v + 16, 8)

    def plane(yy, xx):
        return (m4(yy) * 4 + m4(xx), dp)

    def along(zz):
        return (sp, m8(zz) * 2 + c)

    partner = (sp, z * 2 + (1 - c))
    xp, xm, yp, ym = plane(y, x + 1), plane(y, x - 1), plane(y + 1, x), plane(y - 1, x)
    zp, zm = along(z + 1), along(z - 1)

    local = [
        pltpu.make_async_copy(wkv_hbm, wd.at[z, :, pl.ds(0, RANK)], local_sems.at[0]),
        pltpu.make_async_copy(wq_hbm, wd.at[z, :, pl.ds(RANK, RANK)], local_sems.at[1]),
        pltpu.make_async_copy(tok_hbm, tk, local_sems.at[2]),
        pltpu.make_async_copy(
            wqup_hbm.at[:, pl.ds(pl.multiple_of(y * 768, 128), 768)], wqs, local_sems.at[3]
        ),
        pltpu.make_async_copy(
            wkvup_hbm.at[:, pl.ds(pl.multiple_of(y * 1024, 128), 1024)],
            wup.at[dp, :, pl.ds(Q_WIDTH + R_WIDTH, 1024)],
            local_sems.at[4],
        ),
        pltpu.make_async_copy(
            wout_hbm, wo.at[:, pl.ds(pl.multiple_of(dp * 128, 128), 128)], local_sems.at[5]
        ),
        pltpu.make_async_copy(wrot_hbm, wrot, local_sems.at[6]),
    ]
    for i in range(4):
        local.append(
            pltpu.make_async_copy(
                tab_hbm.at[pl.ds(pl.multiple_of(i * 1024 + x * 256, 256), 256)], tab.at[i], local_sems.at[7 + i]
            )
        )
    for copy in local:
        copy.start()

    moves = []

    def move(src, dst, peer, incoming):
        k = len(moves)
        moves.append(Move((send_sems.at[k], recv_sems.at[k]), src, dst, peer, incoming))
        return moves[-1]

    def ring(view):
        steps = {}
        for s in range(1, 4):
            up, down = view(z - s + 1), view(z + s - 1)
            steps[s] = (move(up, up, zp, view(z - s)), move(down, down, zm, view(z + s)))
        up, down = view(z - 3, 0), view(z + 3, 1)
        steps[4] = (move(up, up, zp, view(z - 4, 0)), move(down, down, zm, view(z + 4, 1)))
        return steps

    colour = m4(x + 2 * y)

    def quarter(ch, zo, q, part=None):
        columns = pl.ds(RANK * ch, RANK)
        if part is None:
            return wd.at[m8(zo), pl.ds(pl.multiple_of(m4(q) * 32, 32), 32), columns]
        return wd.at[m8(zo), pl.ds(pl.multiple_of(m4(q) * 32 + 16 * part, 16), 16), columns]

    def sides_of(ch, zo):
        own = quarter(ch, zo, colour)
        first, second = quarter(ch, zo, colour, 0), quarter(ch, zo, colour, 1)
        return (
            move(own, own, xp, quarter(ch, zo, colour - 1)),
            move(own, own, xm, quarter(ch, zo, colour + 1)),
            move(first, first, yp, quarter(ch, zo, colour + 2, 0)),
            move(second, second, ym, quarter(ch, zo, colour + 2, 1)),
        )

    near = (-1, 1, -2, 2, -3, 3, 4)
    own_quarter = quarter(0, z, colour)
    direct = {d: move(own_quarter, own_quarter, along(z + d), quarter(0, z - d, colour)) for d in near}
    down = ring(lambda zo, part=None: quarter(1, zo, colour, part))
    sides = [{d: sides_of(ch, z + d) for d in near} for ch in range(2)]
    tokens_over = move(tk, pt, partner, pt)
    partial_over = [move(part_send.at[ch], part_recv.at[ch], partner, part_recv.at[ch]) for ch in range(2)]

    def up_block(zo, part=None, core=c):
        if part is None:
            return wup.at[m8(zo) * 2 + core]
        return wup.at[m8(zo) * 2 + core, pl.ds(16 * part, 16)]

    up = ring(up_block)
    up_hand = {
        d: move(up_block(z + d), up_block(z + d), partner, up_block(z + d, core=1 - c))
        for d in (0, -1, 1, -2, 2, -3, 3, 4)
    }

    def out_view(chunk, zo, part=None):
        lo, size = (512 * chunk, 512) if part is None else (512 * chunk + 256 * part, 256)
        return wo.at[pl.ds(lo, size), pl.ds(pl.multiple_of(m8(zo) * 256 + c * 128, 128), 128)]

    def out_column(zo, core):
        return wo.at[:, pl.ds(pl.multiple_of(m8(zo) * 256 + core * 128, 128), 128)]

    out = [ring(functools.partial(out_view, chunk)) for chunk in range(4)]
    out_hand = {
        d: move(out_column(z + d, c), out_column(z + d, c), partner, out_column(z + d, 1 - c))
        for d in (0, -1, 1, -2, 2, -3, 3, 4)
    }

    def hand(hands, step):
        for d in (-step, step) if step < 4 else (4,):
            hands[d].start()

    def out_visit(step, chunk):
        wait_all(out[chunk][step])
        if step < 4:
            start_all(out[chunk][step + 1])
        if chunk == 3:
            hand(out_hand, step)

    mid_a, mid_b = A_ROWS // 2, A_ROWS + (KV_ROWS - A_ROWS) // 2

    def rows_of(spans, oy, ox, part=None):
        lo, hi = spans[0 if part is None else part + 1]
        return kvb.at[m4(oy) * 4 + m4(ox), pl.ds(lo, hi - lo)]

    a_piece = functools.partial(rows_of, ((0, A_ROWS), (0, mid_a), (mid_a, A_ROWS)))
    b_piece = functools.partial(rows_of, ((A_ROWS, KV_ROWS), (A_ROWS, mid_b), (mid_b, KV_ROWS)))

    def q_piece(oy, ox, part=None):
        if part is None:
            return qb.at[m4(oy)]
        return qb.at[m4(oy), pl.ds(128 * part, 128)]

    def x_first(piece, oy):
        own = piece(oy, x)
        return move(own, own, xp, piece(oy, x - 1)), move(own, own, xm, piece(oy, x + 1))

    def x_second(piece, oy):
        left, right = piece(oy, x - 1, 0), piece(oy, x + 1, 1)
        return move(left, left, xp, piece(oy, x - 2, 0)), move(right, right, xm, piece(oy, x + 2, 1))

    def y_first(piece, ox):
        own = piece(y, ox)
        return move(own, own, yp, piece(y - 1, ox)), move(own, own, ym, piece(y + 1, ox))

    def y_second(piece, ox):
        under, over = piece(y - 1, ox, 0), piece(y + 1, ox, 1)
        return move(under, under, yp, piece(y - 2, ox, 0)), move(over, over, ym, piece(y + 2, ox, 1))

    ax1, ax2 = x_first(a_piece, y), x_second(a_piece, y)
    ay1 = {d: y_first(a_piece, x + d) for d in (0, -1, 1, 2)}
    ay2 = {d: y_second(a_piece, x + d) for d in (0, -1, 1, 2)}
    by1, by2 = y_first(b_piece, x), y_second(b_piece, x)
    bx1 = {d: x_first(b_piece, y + d) for d in (0, -1, 1, 2)}
    bx2 = {d: x_second(b_piece, y + d) for d in (0, -1, 1, 2)}
    qy1, qy2 = y_first(q_piece, x), y_second(q_piece, x)
    back = {
        d: move(osend.at[m4(y + d)], orecv.at[y], plane(y + d, x), orecv.at[m4(y - d)]) for d in (2, 1, 3)
    }

    barrier = pltpu.get_barrier_semaphore()
    for peer in (xp, xm, yp, ym, plane(y + 2, x), partner) + tuple(along(z + d) for d in near):
        pl.semaphore_signal(barrier, inc=1, device_id=peer, device_id_type=MESH)
    pl.semaphore_wait(barrier, 13)

    local[0].wait()
    for d in (4, -3, 3, -2, 2, -1, 1):
        direct[d].start()
    local[2].wait()
    tokens_over.start()
    local[1].wait()
    start_all(down[1])

    local[3].wait()
    for h in range(4):
        wup[dp, :, NOPE * h : NOPE * (h + 1)] = wqs[:, 192 * h : 192 * h + NOPE]
    wup[dp, :, Q_WIDTH : Q_WIDTH + R_WIDTH] = jnp.concatenate(
        [wqs[:, 192 * h + NOPE : 192 * (h + 1)] for h in range(4)], axis=1
    )
    local[4].wait()
    start_all(up[1])
    up_hand[0].start()

    def relay(step):
        wait_all(down[step] + up[step])
        if step < 4:
            start_all(down[step + 1] + up[step + 1])
        for d in (-step, step) if step < 4 else (4,):
            start_all(sides[1][d])
        hand(up_hand, step)

    def pass_on(d):
        direct[-d if d != 4 else 4].wait()
        start_all(sides[0][d])

    for copy in local[6:11]:
        copy.wait()
    own_tab = tab[y]
    kr = lax.dot_general(tk[...], wrot[...], (((1,), (1,)), ((), ())), preferred_element_type=F32)
    kr_swap = jnp.concatenate([kr[:, 32:], kr[:, :32]], axis=1)
    kr = (kr * own_tab[:, :64] + kr_swap * own_tab[:, 64:]).astype(BF16)
    packed = jnp.concatenate([kr[:128], kr[128:]], axis=1)
    for t in range(4):
        kvb[sp, BLOCK:KV_ROWS, 128 * t : 128 * (t + 1)] = packed[32 * t : 32 * (t + 1)]

    for d in (-1, 1, -2, 2):
        pass_on(d)
    tokens_over.wait()
    for zo in range(8):
        columns = pl.ds(pl.multiple_of(256 * zo + 128 * c, 128), 128)
        lhs[0:256, 128 * zo : 128 * (zo + 1)] = tk[:, columns]
        lhs[256:512, 128 * zo : 128 * (zo + 1)] = pt[:, columns]
    for d in (-3, 3, 4):
        pass_on(d)
    relay(1)
    for h in range(4):
        vbuf[h, :, :, VDIM:256] = jnp.ones((16, BLOCK, 256 - VDIM), BF16)

    def down_weights(ch):
        return wd[:, :, RANK * ch : RANK * (ch + 1)].reshape(1024, RANK)

    def down_partner(ch):
        for d in near:
            wait_all(sides[ch][d])
        part_send[ch] = dot(lhs[256:512], down_weights(ch))
        partial_over[ch].start()

    def down_own(ch):
        own = dot(lhs[0:256], down_weights(ch))
        partial_over[ch].wait()
        return own + part_recv[ch]

    down_partner(0)
    relay(2)
    kvb[sp, 0:BLOCK, :] = norm(down_own(0), kv_gain[...]).astype(BF16)
    start_all(ax1 + bx1[0] + by1 + ay1[0])
    acc[...] = jnp.zeros_like(acc)
    mbuf[...] = jnp.full_like(mbuf, -jnp.inf)
    relay(3)
    relay(4)
    local[5].wait()
    for chunk in range(4):
        start_all(out[chunk][1])
    wait_all(ax1)
    start_all(ax2 + ay1[-1] + ay1[1])
    wait_all(bx1[0])
    start_all(bx2[0])
    wait_all(by1)
    start_all(by2 + bx1[1] + bx1[-1])
    down_partner(1)
    qb[y] = norm(down_own(1), q_gain[...]).astype(BF16)
    start_all(qy1)

    def expand_queries(i):
        rows = dot(qb[i], wup[:, :, 0 : Q_WIDTH + R_WIDTH].reshape(RANK, Q_WIDTH + R_WIDTH))
        first_half = lax.rem(lax.broadcasted_iota(jnp.int32, (BLOCK, R_WIDTH), 1), 64) < 32
        low = lax.broadcasted_iota(jnp.int32, (BLOCK, 128), 1) < 64
        table = tab[i]
        cosine = jnp.concatenate([table[:, :64]] * 4, axis=1)
        sine = jnp.concatenate([table[:, 64:]] * 4, axis=1)
        u = rows[:, Q_WIDTH:]
        swapped = jnp.where(first_half, pltpu.roll(u, R_WIDTH - 32, 1), pltpu.roll(u, 32, 1))
        turned = u * cosine + swapped * sine
        for h in range(4):
            qcat[h, i, :, 0:NOPE] = rows[:, NOPE * h : NOPE * (h + 1)].astype(BF16)
            pair = turned[:, 128 * (h // 2) : 128 * (h // 2 + 1)]
            keep = low if h % 2 == 0 else jnp.logical_not(low)
            qcat[h, i, :, NOPE:256] = jnp.where(keep, pair, 0.0).astype(BF16)

    def expand_keys(oy, ox, place):
        source, o = m4(oy) * 4 + m4(ox), m4(oy) * 4 + place
        rows = dot(kvb[source, 0:BLOCK, :], wup[:, :, Q_WIDTH + R_WIDTH :].reshape(RANK, 1024)).astype(BF16)
        low = lax.broadcasted_iota(jnp.int32, (32, 128), 1) < 64
        for h in range(4):
            kcat[h, o, :, 0:NOPE] = rows[:, 256 * h : 256 * h + NOPE]
            vbuf[h, o, :, 0:VDIM] = rows[:, 256 * h + NOPE : 256 * (h + 1)]
        for t in range(4):
            pair = kvb[source, BLOCK:KV_ROWS, 128 * t : 128 * (t + 1)].astype(F32)
            turned = pltpu.roll(pair, 64, 1)
            first = jnp.where(low, pair, turned).astype(BF16)
            second = jnp.where(low, turned, pair).astype(BF16)
            for h in range(4):
                kcat[h, o, 32 * t : 32 * (t + 1), NOPE:256] = first
                kcat[h, o, 128 + 32 * t : 128 + 32 * (t + 1), NOPE:256] = second

    def expand_many(which):
        dy, dxs = which

        def step(j, carry):
            expand_keys(y + dy, x + dxs[0] + j * (dxs[-1] - dxs[0]), PLACE[dxs[0]] + j)
            return carry

        lax.fori_loop(0, len(dxs), step, 0)

    wait_all(up_hand.values())
    expand_many((0, (0,)))
    expand_queries(y)
    wait_all(ay1[0])
    start_all(ay2[0])
    wait_all(ax2)
    start_all(ay1[2])
    out_visit(1, 0)
    expand_many((0, (-1, 1)))
    wait_all(qy1)
    start_all(qy2)
    out_visit(1, 1)

    def near_queries(j, carry):
        expand_queries(m4(y - 1 + 2 * j))
        return carry

    lax.fori_loop(0, 2, near_queries, 0)
    wait_all(by2)
    start_all(bx1[2])
    wait_all(bx2[0])
    expand_many((0, (2,)))
    out_visit(1, 2)

    width = BLOCK * KEY_BLOCKS

    def column_of(place):
        return m4(x + jnp.where(place == 1, 3, jnp.where(place == 2, 1, jnp.where(place == 3, 2, 0))))

    def attend(i, r, sub, masked):
        first = 4 * r + KEY_BLOCKS * sub

        def scores_of(h):
            k = kcat[h, pl.ds(first, KEY_BLOCKS)].reshape(width, 256)
            return lax.dot_general(qcat[h, i], k, (((1,), (1,)), ((), ())), preferred_element_type=F32)

        def take(h, s):
            if masked:
                ahead = lax.broadcasted_iota(jnp.int32, (BLOCK, BLOCK), 1) - lax.broadcasted_iota(
                    jnp.int32, (BLOCK, BLOCK), 0
                )
                parts = []
                for b in range(KEY_BLOCKS):
                    limit = BLOCK * (x - column_of(KEY_BLOCKS * sub + b))
                    parts.append(jnp.where(ahead <= limit, s[:, BLOCK * b : BLOCK * (b + 1)], -jnp.inf))
                s = jnp.concatenate(parts, axis=1) if KEY_BLOCKS > 1 else parts[0]
            old = mbuf[h, i]
            top = jnp.maximum(old, jnp.max(s, axis=-1, keepdims=True) * SCALE)
            p = jnp.exp2(s * SCALE - top[:, :1]).astype(BF16)
            alpha = jnp.exp2(old - top)
            mbuf[h, i] = top
            v = vbuf[h, pl.ds(first, KEY_BLOCKS)].reshape(width, 256)
            acc[h, i] = acc[h, i] * jnp.concatenate([alpha, alpha], axis=1) + dot(p, v)

        ahead = scores_of(0)
        for h in range(4):
            s, ahead = ahead, scores_of(h + 1) if h < 3 else None
            take(h, s)

    def finish(i):
        for h in range(4):
            done = acc[h, i]
            osend[i, :, VDIM * h : VDIM * (h + 1)] = (done[:, :VDIM] / done[:, VDIM:]).astype(BF16)

    def at_1():
        wait_all(ay1[-1])
        start_all(ay2[-1])
        wait_all(ay1[1])
        start_all(ay2[1])

    def at_2():
        wait_all(bx1[1])
        start_all(bx2[1])
        wait_all(bx1[-1])
        start_all(bx2[-1])

    def at_3():
        wait_all(qy2)
        expand_queries(m4(y + 2))

    def at_4():
        wait_all(ay1[2])
        start_all(ay2[2])
        expand_many((1, (0,)))
        expand_many((1, (-1, 1)))
        wait_all(bx2[1])
        expand_many((1, (2,)))

    def at_6():
        wait_all(bx1[2])
        start_all(bx2[2])

    def at_8():
        expand_many((-1, (0,)))
        expand_many((-1, (-1, 1)))
        wait_all(bx2[-1])
        expand_many((-1, (2,)))

    def send_back(d):
        finish(m4(y + d))
        back[d].start()

    def at_last(place):
        if place == 0:
            for d in (1, 3):
                pl.when(m4(y + d) < m4(y + 2))(functools.partial(send_back, d))
            wait_all(ay2[0])
            expand_many((2, (0,)))
        elif place == 1:
            wait_all(ay2[-1])
            expand_many((2, (-1,)))
        elif place == 2:
            wait_all(ay2[1])
            expand_many((2, (1,)))
        else:
            wait_all(ay2[2] + bx2[2])
            expand_many((2, (2,)))

    def at_sub(sub):
        for b in range(KEY_BLOCKS):
            at_last(KEY_BLOCKS * sub + b)

    last_row = 12 * SUBS
    events = {1: at_1, 2: at_2, 3: at_3, 4: at_4, 6: at_6, 8: at_8}
    events = {SUBS * at: event for at, event in events.items()}
    events.update({last_row + 4 * sub: functools.partial(at_sub, sub) for sub in range(SUBS)})
    visits = {0: (1, 3), 1: (2, 0), 2: (2, 1), 3: (2, 2), 4: (2, 3), 6: (3, 0), 7: (3, 1), 8: (3, 2), 9: (3, 3)}

    def slot(v, done):
        late = v >= last_row
        rho = jnp.minimum(lax.div(v, 4 * SUBS), 3)
        kappa = jnp.where(late, lax.rem(v, 4), lax.rem(lax.div(v, SUBS), 4))
        sub = jnp.where(late, lax.div(v - last_row, 4), lax.rem(v, SUBS))
        swap = jnp.where(kappa == 2, 3, jnp.where(kappa == 3, 2, kappa))
        dr = jnp.where(rho == 2, 3, jnp.where(rho == 3, 2, rho))
        last = jnp.where(kappa == 0, 2, jnp.where(kappa == 2, 3, jnp.where(kappa == 3, 0, 1)))
        r, i = m4(y + dr), m4(y + jnp.where(late, last, swap))
        for at, event in events.items():
            pl.when(v == at)(event)
        if KEY_BLOCKS == 1:
            column = column_of(sub)
            edge = jnp.logical_and(i == r, column == x)
            whole = jnp.logical_or(i > r, jnp.logical_and(i == r, column < x))
        else:
            edge, whole = i == r, i > r
        pl.when(edge)(lambda: attend(i, r, sub, True))
        pl.when(whole)(lambda: attend(i, r, sub, False))
        active = i >= r
        for number, (step, chunk) in visits.items():
            pl.when(jnp.logical_and(active, done == SUBS * number))(functools.partial(out_visit, step, chunk))
        for at, d in ((0, 2), (1, 1), (2, 3)):
            pl.when(jnp.logical_and(v == last_row + 4 * (SUBS - 1) + at, active))(functools.partial(send_back, d))
        return done + active.astype(jnp.int32)

    lax.fori_loop(0, 16 * SUBS, slot, jnp.int32(0))
    finish(y)

    out_hand[0].start()
    for chunk in range(4):
        out_visit(4, chunk)
    wait_all(out_hand.values())

    def project(attended, j):
        return dot(attended, wo[pl.ds(pl.multiple_of(512 * j, 512), 512), :])

    late = list(back.values()) + list(out_hand.values()) + [each for steps in out for each in steps[4]]
    for each in moves:
        if each not in late:
            each.finish()
    total = project(osend[y], y)
    for d in (3, 1, 2):
        back[d].wait()
        total = total + project(orecv[m4(y - d)], m4(y - d))
    out_ref[...] = norm(total, out_gain[...]).astype(BF16)
    for each in late:
        each.finish()


N_COPIES = 208


def body(tokens, w_qdown, w_kvdown, w_rotary, q_gain, kv_gain, w_qup, w_kvup, w_out, out_gain):
    table = jnp.asarray(turn_table())
    any_spec = pl.BlockSpec(memory_space=pl.ANY)
    vmem_spec = pl.BlockSpec(memory_space=pltpu.VMEM)
    call = pl.pallas_call(
        kernel,
        out_shape=pltpu.VMEM((BLOCK, D), BF16),
        in_specs=[any_spec, any_spec, any_spec, any_spec, vmem_spec, vmem_spec]
        + [any_spec, any_spec, any_spec, vmem_spec, any_spec],
        out_specs=vmem_spec,
        scratch_shapes=[
            pltpu.VMEM((BLOCK, D), BF16),
            pltpu.VMEM((BLOCK, D), BF16),
            pltpu.VMEM((2 * BLOCK, 1024), BF16),
            pltpu.VMEM((8, 128, 1024), BF16),
            pltpu.VMEM((2, BLOCK, RANK), F32),
            pltpu.VMEM((2, BLOCK, RANK), F32),
            pltpu.VMEM((16, KV_ROWS, RANK), BF16),
            pltpu.VMEM((4, BLOCK, RANK), BF16),
            pltpu.VMEM((32, 768), BF16),
            pltpu.VMEM((16, 32, UP_WIDTH), BF16),
            pltpu.VMEM((D, D), BF16),
            pltpu.VMEM((ROPE, D), BF16),
            pltpu.VMEM((4, BLOCK, 128), F32),
            pltpu.VMEM((4, 16, BLOCK, 256), BF16),
            pltpu.VMEM((4, 16, BLOCK, 256), BF16),
            pltpu.VMEM((4, 4, BLOCK, 256), BF16),
            pltpu.VMEM((4, 4, BLOCK, 256), F32),
            pltpu.VMEM((4, 4, BLOCK, 128), F32),
            pltpu.VMEM((4, BLOCK, 512), BF16),
            pltpu.VMEM((4, BLOCK, 512), BF16),
            pltpu.SemaphoreType.DMA((N_COPIES,)),
            pltpu.SemaphoreType.DMA((N_COPIES,)),
            pltpu.SemaphoreType.DMA((11,)),
        ],
        compiler_params=pltpu.CompilerParams(
            collective_id=0, has_side_effects=True, vmem_limit_bytes=58 * 1024 * 1024
        ),
        name="latent_attention",
    )
    mixed = call(
        tokens[0], w_qdown, w_kvdown, w_rotary.T, q_gain[None], kv_gain[None],
        w_qup, w_kvup, w_out, out_gain[None], table,
    )
    return mixed[None]


def solution(mesh):
    in_specs = (
        P("dp", "sp", None),
        P("dp", None),
        P("dp", None),
        P(),
        P(),
        P(),
        P("dp", None),
        P("dp", None),
        P(None, "dp"),
        P(),
    )
    out_specs = P("dp", "sp", None)
    return jax.shard_map(body, mesh=mesh, in_specs=in_specs, out_specs=out_specs, check_vma=False)
```
